256 devices in a mesh: sp: 32 (over z, y), fs: 4 (over x), tp: 2 (over core).
Axes of the slice: x: 4, y: 4, z: 8, core: 2. Of those that a mesh axis runs over, the one named last changes fastest.
Arguments:
- hidden_in: bfloat16 [4, 8192, 2048], P('fs', 'sp', 'tp'), may hold values from -6 to 6
- sb_query_w: bfloat16 [2048, 1024], P('fs', 'tp'), may hold values from -0.21875 to 0.21875
- sb_key_w: bfloat16 [2048, 1024], P('fs', 'tp'), may hold values from -0.21875 to 0.21875
- sb_value_w: bfloat16 [2048, 1024], P('fs', 'tp'), may hold values from -0.125 to 0.125
- sb_offset: float32 [16], P('tp'), may hold values from -16 to -6
- delta_query_w: bfloat16 [2048, 1024], P('fs', 'tp'), may hold values from -0.125 to 0.125
- delta_key_w: bfloat16 [2048, 1024], P('fs', 'tp'), may hold values from -0.125 to 0.125
- delta_value_w: bfloat16 [2048, 1024], P('fs', 'tp'), may hold values from -0.125 to 0.125
- decay_w: bfloat16 [2048, 8], P(None, 'tp'), may hold values from -0.125 to 0.125
- write_w: bfloat16 [2048, 8], P(None, 'tp'), may hold values from -0.125 to 0.125
- write_bias: float32 [8], P('tp'), may hold values from -7 to 1.5
- decay_log_scale: float32 [8], P('tp'), may hold values from -14 to -3
- decay_shift: float32 [4, 8, 8192], P('fs', 'tp', 'sp'), may hold values from -3 to 0
- head_gain: float32 [128], replicated, may hold values from 0.1 to 1.9
- sb_out_w: bfloat16 [1024, 2048], P('tp'), may hold values from -0.125 to 0.125
- delta_out_w: bfloat16 [1024, 2048], P('tp'), may hold values from -0.125 to 0.125
Outputs:
- mixed_out: bfloat16 [4, 8192, 2048], P('fs', ('sp', 'tp'))
The draws below stay inside these ranges and needn't reach their ends.
All inputs are finite; a program needn't handle non-finite values.
Results may differ from the reference program's by a relative error of at most 0.015.
Values may be sent and summed in bfloat16 or wider, within the bound.
A program may use at most 128 MiB of HBM per device.

```python
import jax
import jax.numpy as jnp
from jax import lax

D = 2048
SB_HEADS = 16
SB_DIM = 64
GDN_HEADS = 8
GDN_DIM = 128
BLOCK = 64
TOK_DEV = 256
LEN = 8192
SEQS = 4
N_TP = 2


def head_kinds(key, fast_share):
    return jax.random.uniform(jax.random.fold_in(key, 71), (GDN_HEADS,), jnp.float32) < fast_share


def draw_sb_offset(key, part):
    reach_term = jax.random.uniform(key, (SB_HEADS,), jnp.float32, -1.0, 2.5)
    return reach_term - jnp.log(jnp.float32(LEN)) - 4.5


def draw_write_bias(key, part):
    fast_share = 0.5
    chosen = head_kinds(key, fast_share)
    strong_term = jax.random.uniform(jax.random.fold_in(key, 5), (GDN_HEADS,), jnp.float32, -1.0, 1.5)
    faint_summand = jax.random.uniform(jax.random.fold_in(key, 6), (GDN_HEADS,), jnp.float32, -7.0, -5.5)
    return jnp.where(chosen, strong_term, faint_summand)


def draw_decay_log_scale(key, part):
    split_keys = jax.random.split(key, 3)
    fast_share = 0.5
    chosen = head_kinds(key, fast_share)
    fast_rate = jax.random.uniform(split_keys[1], (GDN_HEADS,), jnp.float32, 0.015, 0.04)
    slow_rate = jax.random.uniform(split_keys[2], (GDN_HEADS,), jnp.float32, 2e-06, 8e-06)
    return jnp.log(jnp.where(chosen, fast_rate, slow_rate))


def draw_decay_shift(key, part):
    split_keys = jax.random.split(key, 3)
    blocks_count = LEN // TOK_DEV
    minimal_level = 0.15
    highest = 1.2
    rates = jnp.exp(jax.random.uniform(split_keys[0], (SEQS, GDN_HEADS, blocks_count), jnp.float32, jnp.log(minimal_level), jnp.log(highest)))
    unweighted_result = jnp.repeat(rates, TOK_DEV, axis=2) * (-1.0 / LEN)
    destination_indices = jax.random.randint(split_keys[1], (SEQS, GDN_HEADS, 3), 0, LEN)
    forgetting_amounts = jnp.log(jax.random.uniform(split_keys[2], (SEQS, GDN_HEADS, 3), jnp.float32, 0.5, 0.8))
    cell_locations = jnp.arange(LEN, dtype=jnp.int32)
    storing_pulses = jnp.sum(jnp.where(cell_locations[None, None, None, :] == destination_indices[..., None], forgetting_amounts[..., None], 0.0), axis=2)
    return unweighted_result + storing_pulses


def shard_levels(own_key, dims, pieces, smallest, top_value):
    gain, own = 1.0, jax.random.fold_in(own_key, 6)
    for axis_at, blocks in pieces:
        heights = jnp.exp(jax.random.uniform(jax.random.fold_in(own, axis_at), (blocks,), jnp.float32, smallest / len(pieces), top_value / len(pieces)))
        gain = gain * jnp.repeat(heights, dims[axis_at] // blocks).reshape([-1 if axis == axis_at else 1 for axis in range(len(dims))])
    return gain


def gaussian(own_key, dims, scale, reach, shards=(), kind=jnp.bfloat16):
    drawn = jax.random.normal(own_key, dims, jnp.float32) * scale
    if len(shards) > 0:
        drawn = shard_levels(own_key, dims, shards, -0.22, 0.18) * drawn
    return jnp.clip(drawn, min=-reach, max=reach).astype(kind)


def setup_inputs(seed: int = 0) -> dict:
    streams_of = jax.random.split(jax.random.key(seed), 17)
    hidden_in = gaussian(streams_of[0], (SEQS, LEN, D), 1.0, 6.0, ((0, 4), (1, 32), (2, 2)))
    sb_query_w = gaussian(streams_of[1], (D, SB_HEADS * SB_DIM), (D // 3) ** -0.5, 0.21875, ((0, 4), (1, 2)))
    sb_key_w = gaussian(streams_of[2], (D, SB_HEADS * SB_DIM), (D // 3) ** -0.5, 0.21875, ((0, 4), (1, 2)))
    sb_value_w = gaussian(streams_of[3], (D, SB_HEADS * SB_DIM), D ** -0.5, 0.125, ((0, 4), (1, 2)))
    sb_offset = draw_sb_offset(jax.random.fold_in(streams_of[16], 71), 0)
    delta_query_w = gaussian(streams_of[5], (D, GDN_HEADS * GDN_DIM), D ** -0.5, 0.125, ((0, 4), (1, 2)))
    delta_key_w = gaussian(streams_of[6], (D, GDN_HEADS * GDN_DIM), D ** -0.5, 0.125, ((0, 4), (1, 2)))
    delta_value_w = gaussian(streams_of[7], (D, GDN_HEADS * GDN_DIM), D ** -0.5, 0.125, ((0, 4), (1, 2)))
    decay_w = gaussian(streams_of[8], (D, GDN_HEADS), D ** -0.5, 0.125, ((1, 2),))
    write_w = gaussian(streams_of[9], (D, GDN_HEADS), D ** -0.5, 0.125, ((1, 2),))
    write_bias = draw_write_bias(jax.random.fold_in(streams_of[16], 71), 0)
    decay_log_scale = draw_decay_log_scale(jax.random.fold_in(streams_of[16], 71), 0)
    decay_shift = draw_decay_shift(jax.random.fold_in(streams_of[16], 71), 0)
    head_gain = jnp.clip(1.0 + 0.18 * jax.random.normal(streams_of[13], (GDN_DIM,), jnp.float32), 0.1, 1.9)
    sb_out_w = gaussian(streams_of[14], (SB_HEADS * SB_DIM, D), (SB_HEADS * SB_DIM + GDN_HEADS * GDN_DIM) ** -0.5, 0.125, ((0, 2),))
    delta_out_w = gaussian(streams_of[15], (GDN_HEADS * GDN_DIM, D), (SB_HEADS * SB_DIM + GDN_HEADS * GDN_DIM) ** -0.5, 0.125, ((0, 2),))
    return dict(hidden_in=hidden_in, sb_query_w=sb_query_w, sb_key_w=sb_key_w, sb_value_w=sb_value_w, sb_offset=sb_offset, delta_query_w=delta_query_w, delta_key_w=delta_key_w, delta_value_w=delta_value_w, decay_w=decay_w, write_w=write_w, write_bias=write_bias, decay_log_scale=decay_log_scale, decay_shift=decay_shift, head_gain=head_gain, sb_out_w=sb_out_w, delta_out_w=delta_out_w)


EXACT_MATMUL = lax.Precision.HIGHEST
NORM_EPS = 1e-06

def unit_lower_inverse(strict_part):
    order_size = strict_part.shape[-1]
    powered = strict_part
    inverse = jnp.eye(order_size, dtype=strict_part.dtype) - strict_part
    for repeat_number in range(max(1, (order_size - 1).bit_length()) - 1):
        powered = jnp.einsum('...ij,...jk->...ik', powered, powered, precision=EXACT_MATMUL)
        inverse = inverse + jnp.einsum('...ij,...jk->...ik', inverse, powered, precision=EXACT_MATMUL)
    return inverse

def to_blocks(row_data, block_span):
    blocks_count = row_data.shape[0] // block_span
    shaped = row_data.reshape((blocks_count, block_span) + row_data.shape[1:])
    return jnp.swapaxes(shaped, 1, 2)

def from_blocks(blocked):
    swapped = jnp.swapaxes(blocked, 1, 2)
    return swapped.reshape((-1,) + swapped.shape[2:])

def unit_rows(vectors):
    return vectors * lax.rsqrt(lax.optimization_barrier(jnp.sum(vectors * vectors, axis=-1, keepdims=True)) + NORM_EPS)

def delta_inputs(query_proj, key_proj, value_proj, decay_pre, write_pre, write_bias, decay_log_scale, shift_rows, head_count, head_size):
    query_act = jax.nn.silu(query_proj.astype(jnp.float32)).reshape(-1, head_count, head_size)
    key_act = jax.nn.silu(key_proj.astype(jnp.float32)).reshape(-1, head_count, head_size)
    value_rows = jax.nn.silu(value_proj.astype(jnp.float32)).reshape(-1, head_count, head_size)
    queries = unit_rows(query_act) * head_size ** (-0.5)
    key_rows = unit_rows(key_act)
    log_decay = -jnp.exp(decay_log_scale) * jax.nn.softplus(decay_pre) + shift_rows
    strength = jax.nn.sigmoid(write_pre + write_bias)
    return (queries, key_rows, value_rows, log_decay, strength)

def delta_prepare(queries, key_rows, value_rows, log_decay, strength):
    block_span = queries.shape[2]
    cumulative = jnp.cumsum(log_decay, axis=-1)
    row_place = lax.broadcasted_iota(jnp.int32, (block_span, block_span), 0)
    col_place = lax.broadcasted_iota(jnp.int32, (block_span, block_span), 1)
    inclusive = col_place <= row_place
    strictly = col_place < row_place
    spread = cumulative[..., :, None] - cumulative[..., None, :]
    decay_table = jnp.where(inclusive, jnp.exp(jnp.where(inclusive, spread, 0.0)), 0.0)
    keys_beta = key_rows * strength[..., None]
    lower_part = jnp.where(strictly, jnp.einsum('nhik,nhjk->nhij', keys_beta, key_rows, precision=EXACT_MATMUL) * decay_table, 0.0)
    inverse = unit_lower_inverse(lower_part)
    growth = jnp.exp(cumulative)
    state_updates = jnp.einsum('nhij,nhjv->nhiv', inverse, value_rows * strength[..., None], precision=EXACT_MATMUL)
    erase_term = jnp.einsum('nhij,nhjk->nhik', inverse, keys_beta * growth[..., None], precision=EXACT_MATMUL)
    inside_block = jnp.einsum('nhik,nhjk->nhij', queries, key_rows, precision=EXACT_MATMUL) * decay_table
    boosted_query = queries * growth[..., None]
    damped_keys = key_rows * jnp.exp(cumulative[..., -1:] - cumulative)[..., None]
    decay_per_block = jnp.exp(cumulative[..., -1])
    return (state_updates, erase_term, inside_block, boosted_query, damped_keys, decay_per_block)

def delta_step(memory_state, inputs):
    state_updates, erase_term, inside_block, boosted_query, damped_keys, decay_per_block = inputs
    fixed_values = state_updates - jnp.einsum('mzq,mqc->mzc', erase_term, memory_state, precision=EXACT_MATMUL)
    produced_rows = jnp.einsum('mzq,mqc->mzc', boosted_query, memory_state, precision=EXACT_MATMUL) + jnp.einsum('efq,eqn->efn', inside_block, fixed_values, precision=EXACT_MATMUL)
    memory_state = memory_state * decay_per_block[:, None, None] + jnp.einsum('wam,waz->wmz', damped_keys, fixed_values, precision=EXACT_MATMUL)
    return (memory_state, produced_rows)

def stick_block(queries, key_rows, value_rows, query_place, key_place, offsets):
    scale_factor = queries.shape[-1] ** (-0.5)
    scores = jnp.einsum('qhd,khd->hqk', queries.astype(jnp.float32), key_rows.astype(jnp.float32)) * scale_factor + offsets[:, None, None]
    visible = key_place[None, :] < query_place[:, None]
    skipped = jnp.where(visible, jax.nn.log_sigmoid(-scores), 0.0)
    beyond = lax.cumsum(skipped, axis=2, reverse=True) - skipped
    weights = jnp.where(visible, jnp.exp(jax.nn.log_sigmoid(scores) + beyond), 0.0).astype(jnp.bfloat16)
    weights = lax.optimization_barrier(weights).astype(jnp.float32)
    partial_value = jnp.einsum('hqk,khd->qhd', weights, value_rows.astype(jnp.float32))
    return (partial_value, lax.optimization_barrier(jnp.sum(skipped, axis=2)).T)

def stick_combine(partials, totals):
    beyond = jnp.cumsum(totals[::-1], axis=0)[::-1] - totals
    return lax.optimization_barrier(jnp.sum(partials * jnp.exp(beyond)[..., None], axis=0))

def stick_sequence(queries, key_rows, value_rows, offsets):
    blocks_count = LEN // TOK_DEV
    query_blocks = queries.reshape((blocks_count, TOK_DEV) + queries.shape[1:])
    key_blocks = key_rows.reshape((blocks_count, TOK_DEV) + key_rows.shape[1:])
    value_blocks = value_rows.reshape((blocks_count, TOK_DEV) + value_rows.shape[1:])
    cell_locations = jnp.arange(LEN, dtype=jnp.int32).reshape(blocks_count, TOK_DEV)
    head_count = queries.shape[1]
    head_size = value_rows.shape[2]

    def per_query(query_index):

        def per_key(key_index):

            def active(unused_arg):
                return stick_block(query_blocks[query_index], key_blocks[key_index], value_blocks[key_index], cell_locations[query_index], cell_locations[key_index], offsets)

            def inactive(unused_arg):
                return (jnp.zeros((TOK_DEV, head_count, head_size), jnp.float32), jnp.zeros((TOK_DEV, head_count), jnp.float32))
            return lax.cond(key_index <= query_index, active, inactive, 0)
        partials, totals = lax.map(per_key, jnp.arange(blocks_count, dtype=jnp.int32))
        return stick_combine(partials, totals)
    gathered = lax.map(per_query, jnp.arange(blocks_count, dtype=jnp.int32))
    return gathered.reshape(LEN, head_count, head_size)

def reference(hidden_in, sb_query_w, sb_key_w, sb_value_w, sb_offset, delta_query_w, delta_key_w, delta_value_w, decay_w, write_w, write_bias, decay_log_scale, decay_shift, head_gain, sb_out_w, delta_out_w):

    def one_sequence(inputs):
        sequence_rows, shift_rows = inputs

        def project(weight):
            return jnp.dot(sequence_rows, weight, preferred_element_type=jnp.float32).astype(jnp.bfloat16)
        sb_query = project(sb_query_w).reshape(LEN, SB_HEADS, SB_DIM)
        sb_keys = project(sb_key_w).reshape(LEN, SB_HEADS, SB_DIM)
        sb_values = project(sb_value_w).reshape(LEN, SB_HEADS, SB_DIM)
        sb_mixed = stick_sequence(sb_query, sb_keys, sb_values, sb_offset).astype(jnp.bfloat16).reshape(LEN, SB_HEADS * SB_DIM)
        decay_pre = jnp.dot(sequence_rows, decay_w, preferred_element_type=jnp.float32)
        write_pre = jnp.dot(sequence_rows, write_w, preferred_element_type=jnp.float32)
        queries, key_rows, value_rows, log_decay, strength = delta_inputs(project(delta_query_w), project(delta_key_w), project(delta_value_w), decay_pre, write_pre, write_bias, decay_log_scale, shift_rows.T, GDN_HEADS, GDN_DIM)
        prepared = delta_prepare(to_blocks(queries, BLOCK), to_blocks(key_rows, BLOCK), to_blocks(value_rows, BLOCK), to_blocks(log_decay, BLOCK), to_blocks(strength, BLOCK))
        initial = jnp.zeros((GDN_HEADS, GDN_DIM, GDN_DIM), jnp.float32)
        unused_memory, produced_rows = lax.scan(delta_step, initial, prepared)
        produced_rows = from_blocks(produced_rows)
        normed = produced_rows * lax.rsqrt(lax.optimization_barrier(jnp.mean(produced_rows * produced_rows, axis=-1, keepdims=True)) + NORM_EPS) * head_gain
        delta_mixed = normed.astype(jnp.bfloat16).reshape(LEN, GDN_HEADS * GDN_DIM)
        sb_group = SB_HEADS * SB_DIM // N_TP
        delta_group = GDN_HEADS * GDN_DIM // N_TP
        accumulated = jnp.zeros((LEN, D), jnp.float32)
        for group_number in range(N_TP):
            sb_cols = slice(group_number * sb_group, (group_number + 1) * sb_group)
            delta_cols = slice(group_number * delta_group, (group_number + 1) * delta_group)
            term = jnp.dot(sb_mixed[:, sb_cols], sb_out_w[sb_cols], preferred_element_type=jnp.float32) + jnp.dot(delta_mixed[:, delta_cols], delta_out_w[delta_cols], preferred_element_type=jnp.float32)
            rounded = lax.optimization_barrier(term.astype(jnp.bfloat16))
            accumulated = accumulated + rounded.astype(jnp.float32)
        return accumulated.astype(jnp.bfloat16)
    return lax.map(one_sequence, (hidden_in, decay_shift))
```

```python
import jax
import jax.numpy as jnp
from jax import lax
from jax.sharding import Mesh
from jax.experimental import pallas as pl
from jax.experimental.pallas import tpu as pltpu
from jax.sharding import PartitionSpec as P

SB_DIM = 64
GDN_DIM = 128
BLOCK = 64
SP = ("sp_0", "sp_1")
SP_TP = ("sp_0", "sp_1", "tp")


NORM_EPS = 1e-06


def joined_along(tiles, dim):
    tiles = jnp.moveaxis(tiles, 0, dim)
    shape = tiles.shape
    return tiles.reshape(*shape[:dim], shape[dim] * shape[dim + 1], *shape[dim + 2 :])


def sent_to_all(value, axis):
    devices = lax.axis_size(axis)
    return lax.all_to_all(
        jnp.broadcast_to(value[None], (devices, *value.shape)), axis, 0, 0, tiled=True
    )


def gathered_copies(value, axis, dim):
    return joined_along(sent_to_all(value, axis), dim)


def in_one_piece(arrays, axis, dim, along):
    widths = [a.shape[along] for a in arrays]
    both = jnp.concatenate(arrays, axis=along)
    result = lax.all_gather(both, axis, axis=dim, tiled=True)
    return tuple(jnp.split(result, [sum(widths[:k]) for k in range(1, len(widths))], axis=along))


def neutral_like(value, identity):
    return jax.tree.map(
        lambda part, zero: jnp.zeros_like(part) + jnp.asarray(zero, part.dtype), value, identity
    )


def entering(value, axes, combine, identity):
    before = start = neutral_like(value, identity)
    so_far = value
    for axis in reversed(axes):
        devices, index = (lax.axis_size(axis), lax.axis_index(axis))
        pieces = jax.tree.map(
            lambda part, kind: lax.all_gather(part.astype(kind), axis),
            so_far,
            (jnp.bfloat16, jnp.bfloat16),
        )
        inside, so_far = (start, start)
        for k in range(devices):
            passed = k < index
            so_far = combine(
                so_far, jax.tree.map(lambda part, own: part[k].astype(own.dtype), pieces, value)
            )
            inside = jax.tree.map(lambda new, old: jnp.where(passed, new, old), so_far, inside)
        before = combine(inside, before)
    return before


def split_up(value, dim, devices):
    before, after = (value.shape[:dim], value.shape[dim + 1 :])
    return jnp.moveaxis(value.reshape(*before, devices, -1, *after), dim, 0)


def sent_and_summed(value, axis, dim):
    tiles = split_up(value, dim, lax.axis_size(axis))
    arrived = lax.all_to_all(tiles, axis, split_axis=0, concat_axis=0, tiled=True)
    return arrived.astype(jnp.float32).sum(axis=0)


def unit_lower_inverse(strict_part):
    order_size = strict_part.shape[-1]
    powered = strict_part
    inverse = jnp.eye(order_size, dtype=strict_part.dtype) - strict_part
    for repeat_number in range(max(1, (order_size - 1).bit_length()) - 1):
        powered = jnp.einsum("...ij,...jk->...ik", powered, powered)
        inverse = inverse + jnp.einsum("...ij,...jk->...ik", inverse, powered)
    return inverse


def to_blocks(row_data, block_span):
    blocks_count = row_data.shape[0] // block_span
    shaped = row_data.reshape((blocks_count, block_span) + row_data.shape[1:])
    return jnp.swapaxes(shaped, 1, 2)


def from_blocks(blocked):
    swapped = jnp.swapaxes(blocked, 1, 2)
    return swapped.reshape((-1,) + swapped.shape[2:])


def unit_rows(vectors):
    return vectors * lax.rsqrt(jnp.sum(vectors * vectors, axis=-1, keepdims=True) + NORM_EPS)


def delta_inputs(
    query_proj,
    key_proj,
    value_proj,
    decay_pre,
    write_pre,
    write_bias,
    decay_log_scale,
    shift_rows,
    head_count,
    head_size,
):
    query_act = jax.nn.silu(query_proj.astype(jnp.float32)).reshape(-1, head_count, head_size)
    key_act = jax.nn.silu(key_proj.astype(jnp.float32)).reshape(-1, head_count, head_size)
    value_rows = jax.nn.silu(value_proj.astype(jnp.float32)).reshape(-1, head_count, head_size)
    queries = unit_rows(query_act) * head_size ** (-0.5)
    key_rows = unit_rows(key_act)
    log_decay = -jnp.exp(decay_log_scale) * jax.nn.softplus(decay_pre) + shift_rows
    strength = jax.nn.sigmoid(write_pre + write_bias)
    return (queries, key_rows, value_rows, log_decay, strength)


def delta_prepare(queries, key_rows, value_rows, log_decay, strength):
    block_span = queries.shape[2]
    cumulative = jnp.cumsum(log_decay, axis=-1)
    row_place = lax.broadcasted_iota(jnp.int32, (block_span, block_span), 0)
    col_place = lax.broadcasted_iota(jnp.int32, (block_span, block_span), 1)
    inclusive = col_place <= row_place
    strictly = col_place < row_place
    spread = cumulative[..., :, None] - cumulative[..., None, :]
    decay_table = jnp.where(inclusive, jnp.exp(jnp.where(inclusive, spread, 0.0)), 0.0)
    keys_beta = key_rows * strength[..., None]
    lower_part = jnp.where(
        strictly, jnp.einsum("nhik,nhjk->nhij", keys_beta, key_rows) * decay_table, 0.0
    )
    inverse = unit_lower_inverse(lower_part)
    growth = jnp.exp(cumulative)
    state_updates = jnp.einsum("nhij,nhjv->nhiv", inverse, value_rows * strength[..., None])
    erase_term = jnp.einsum("nhij,nhjk->nhik", inverse, keys_beta * growth[..., None])
    inside_block = jnp.einsum("nhik,nhjk->nhij", queries, key_rows) * decay_table
    boosted_query = queries * growth[..., None]
    damped_keys = key_rows * jnp.exp(cumulative[..., -1:] - cumulative)[..., None]
    decay_per_block = jnp.exp(cumulative[..., -1])
    return (state_updates, erase_term, inside_block, boosted_query, damped_keys, decay_per_block)


def delta_step(memory_state, inputs):
    state_updates, erase_term, inside_block, boosted_query, damped_keys, decay_per_block = inputs
    fixed_values = state_updates - jnp.einsum("mzq,mqc->mzc", erase_term, memory_state)
    produced_rows = jnp.einsum("mzq,mqc->mzc", boosted_query, memory_state) + jnp.einsum(
        "efq,eqn->efn", inside_block, fixed_values
    )
    memory_state = memory_state * decay_per_block[:, None, None] + jnp.einsum(
        "wam,waz->wmz", damped_keys, fixed_values
    )
    return (memory_state, produced_rows)


def transition_step(carried, inputs):
    memory_state, transfer = carried
    state_updates, erase_term, inside_block, boosted_query, damped_keys, decay_per_block = inputs
    fixed_values = state_updates - jnp.einsum("mzq,mqc->mzc", erase_term, memory_state)
    coupling = jnp.einsum("hik,hil->hkl", damped_keys, erase_term)
    memory_state = memory_state * decay_per_block[:, None, None] + jnp.einsum(
        "wam,waz->wmz", damped_keys, fixed_values
    )
    transfer = transfer * decay_per_block[:, None, None] - jnp.einsum(
        "hkl,hlm->hkm", coupling, transfer
    )
    return ((memory_state, transfer), None)


def compose(prior_blocks, following_blocks):
    joined_map = jnp.einsum("hkl,hlm->hkm", following_blocks[0], prior_blocks[0])
    joined_state = (
        jnp.einsum("djo,dog->djg", following_blocks[0], prior_blocks[1]) + following_blocks[1]
    )
    return (joined_map, joined_state)


def stick_kernel(offset_ref, query_ref, kv_ref, out_ref, later_ref, rows_ref, acc_ref, beyond_ref):
    place = lax.axis_index("sp_1")
    tile = query_ref.shape[2]
    size = query_ref.shape[1]
    groups = kv_ref.shape[2] // tile
    row_at = lax.broadcasted_iota(jnp.int32, (tile, tile), 0)
    col_at = lax.broadcasted_iota(jnp.int32, (tile, tile), 1)
    later_ref[...] = jnp.where(row_at > col_at, 1.0, 0.0).astype(jnp.bfloat16)
    offset = offset_ref[0]

    def key_row(row, blocks, diagonal):
        queries = rows_ref[...]
        beyond = None if diagonal else beyond_ref[...]
        weights = []
        for k in range(blocks - 1, -1, -1):
            scores = (
                jnp.dot(
                    queries,
                    kv_ref[row, 0:size, k * tile : (k + 1) * tile],
                    preferred_element_type=jnp.float32,
                )
                + offset
            )
            above = jnp.maximum(scores, 0.0)
            below = scores - above
            small = jnp.exp(below - above)
            log_term = jnp.where(small < 2.0**-12, small, jnp.log(1.0 + small))
            passed = above + log_term
            exponent = below - log_term
            if diagonal and k == blocks - 1:
                visible = col_at < row_at
                passed = jnp.where(visible, passed, 0.0)
                exponent = jnp.where(visible, exponent, -jnp.inf)
            after = jnp.dot(
                passed.astype(jnp.bfloat16), later_ref[...], preferred_element_type=jnp.float32
            )
            exponent = exponent - after
            if beyond is not None:
                exponent = exponent - beyond
            total = after[:, :1] + passed[:, :1]
            beyond = total if beyond is None else beyond + total
            weights.append(jnp.exp(exponent).astype(jnp.bfloat16))
        partial = lax.dot_general(
            jnp.concatenate(weights[::-1], axis=1),
            kv_ref[row, size : 2 * size, 0 : blocks * tile],
            (((1,), (1,)), ((), ())),
            preferred_element_type=jnp.float32,
        )
        beyond_ref[...] = beyond
        if diagonal:
            acc_ref[...] = partial
        else:
            acc_ref[...] += partial

    def per_query(query_row, unused):
        rows_ref[...] = (
            (query_ref[query_row].astype(jnp.float32) * size ** (-0.5)).T.astype(jnp.bfloat16)
        )
        for k in range(groups):

            @pl.when(place == k)
            def _():
                key_row(query_row, k + 1, True)

        def earlier(step, carried):
            key_row(query_row - 1 - step, groups, False)
            return carried

        lax.fori_loop(0, query_row, earlier, 0)
        out_ref[query_row] = acc_ref[...].T.astype(jnp.bfloat16)
        return unused

    lax.fori_loop(0, query_ref.shape[0], per_query, 0)


def stick_attention(offset, queries, keys_values):
    rows, size, tile = queries.shape
    return pl.pallas_call(
        stick_kernel,
        out_shape=jax.ShapeDtypeStruct((rows, size, tile), jnp.bfloat16),
        in_specs=[
            pl.BlockSpec(memory_space=pltpu.SMEM),
            pl.BlockSpec(memory_space=pltpu.VMEM),
            pl.BlockSpec(memory_space=pltpu.VMEM),
        ],
        out_specs=pl.BlockSpec(memory_space=pltpu.VMEM),
        scratch_shapes=[
            pltpu.VMEM((tile, tile), jnp.bfloat16),
            pltpu.VMEM((tile, size), jnp.bfloat16),
            pltpu.VMEM((tile, size), jnp.float32),
            pltpu.VMEM((tile, 1), jnp.float32),
        ],
        name="stick",
        cost_estimate=pl.CostEstimate(
            flops=40_000_000_000, bytes_accessed=3_000_000, transcendentals=27_000_000
        ),
    )(offset, queries, keys_values)


def on_device(
    hidden_in,
    sb_query_w,
    sb_key_w,
    sb_value_w,
    sb_offset,
    delta_query_w,
    delta_key_w,
    delta_value_w,
    decay_w,
    write_w,
    write_bias,
    decay_log_scale,
    decay_shift,
    head_gain,
    sb_out_w,
    delta_out_w,
):
    tokens, part = hidden_in.shape[1], hidden_in.shape[2]
    fs_count = lax.axis_size("fs")
    sp_count = lax.axis_size(SP)
    z_count = lax.axis_size("sp_0")
    mine = lax.axis_index("fs")
    wide = lax.all_gather(hidden_in.reshape(tokens, part), ("fs", "tp"), axis=0, tiled=False)
    wide = wide.reshape(fs_count, -1, tokens, part)
    rows = sb_query_w.shape[0]
    slab = rows // sp_count
    first = lax.axis_index(SP) * slab
    weights = (sb_query_w, sb_key_w, sb_value_w, delta_query_w, delta_key_w, delta_value_w)
    pieces = jnp.stack([lax.dynamic_slice_in_dim(w, first, slab, 0) for w in weights], axis=1)
    pieces = pieces.reshape(slab, len(weights), fs_count, -1).transpose(2, 0, 1, 3)
    pieces = lax.all_to_all(pieces, "fs", 0, 0, tiled=True)
    pieces = pieces.reshape(fs_count, slab, -1)
    columns = lax.all_gather(pieces, SP, axis=0, tiled=False)
    columns = columns.transpose(1, 0, 2, 3).reshape(wide.shape[1], part, -1)
    gates_w = jnp.concatenate(
        [lax.dynamic_slice_in_dim(w, mine, 1, 1) for w in (decay_w, write_w)], axis=1
    ).reshape(wide.shape[1], part, 2)
    projected = jnp.einsum(
        "ftnc,tcm->fnm", wide, columns, preferred_element_type=jnp.float32
    ).astype(jnp.bfloat16)
    gates = jnp.einsum("ftnc,tcm->mnf", wide, gates_w, preferred_element_type=jnp.float32)
    width = projected.shape[2] // 2
    head_pair = sb_offset.shape[0] // fs_count
    units = (
        projected[:, :, :width]
        .reshape(fs_count, tokens, 3, head_pair, SB_DIM)
        .transpose(0, 3, 2, 4, 1)
        .reshape(z_count, 3 * SB_DIM, tokens)
    )
    arrived = lax.all_to_all(units, "sp_0", 0, 0, tiled=True)
    keys_values = lax.all_gather(arrived[:, SB_DIM:], "sp_1", axis=2, tiled=True)
    offset = lax.dynamic_slice_in_dim(
        sb_offset, head_pair * mine + lax.rem(lax.axis_index("sp_0"), head_pair), 1, 0
    )
    sb_out = stick_attention(offset, arrived[:, :SB_DIM], keys_values)
    dq, dk, dv = (
        projected[:, :, width + k * GDN_DIM : width + (k + 1) * GDN_DIM]
        .transpose(1, 0, 2)
        .reshape(tokens, fs_count * GDN_DIM)
        for k in range(3)
    )
    shift_rows = lax.all_to_all(
        decay_shift.reshape(decay_log_scale.shape[0], tokens), "fs", 0, 0, tiled=True
    ).T
    own_bias = jnp.broadcast_to(lax.dynamic_slice_in_dim(write_bias, mine, 1, 0), (fs_count,))
    own_scale = jnp.broadcast_to(
        lax.dynamic_slice_in_dim(decay_log_scale, mine, 1, 0), (fs_count,)
    )
    queries, key_rows, value_rows, log_decay, strength = delta_inputs(
        dq, dk, dv, gates[0], gates[1], own_bias, own_scale, shift_rows, fs_count, GDN_DIM
    )
    prepared = delta_prepare(
        to_blocks(queries, BLOCK),
        to_blocks(key_rows, BLOCK),
        to_blocks(value_rows, BLOCK),
        to_blocks(log_decay, BLOCK),
        to_blocks(strength, BLOCK),
    )
    identity_map = jnp.broadcast_to(
        jnp.eye(GDN_DIM, dtype=jnp.float32), (fs_count, GDN_DIM, GDN_DIM)
    )
    empty_state = jnp.zeros((fs_count, GDN_DIM, GDN_DIM), jnp.float32)
    (local_end, local_map), unused_out = lax.scan(
        transition_step, (empty_state, identity_map), prepared
    )
    unused_map, incoming = entering(
        (local_map, local_end), SP, compose, (identity_map, empty_state)
    )
    unused_end, produced_rows = lax.scan(delta_step, incoming, prepared)
    produced_rows = from_blocks(produced_rows)
    normed = (
        produced_rows
        * lax.rsqrt(jnp.mean(produced_rows * produced_rows, axis=-1, keepdims=True) + NORM_EPS)
        * head_gain
    )
    delta_mixed = lax.all_to_all(
        normed.astype(jnp.bfloat16).transpose(1, 0, 2), "fs", 0, 0, tiled=True
    )
    sb_back = lax.all_to_all(sb_out, "sp_0", 0, 0, tiled=True)
    sb_mixed = lax.all_to_all(
        sb_back.reshape(fs_count, head_pair * SB_DIM, tokens), "fs", 0, 0, tiled=True
    ).reshape(-1, tokens)
    result = sent_and_summed(
        (
            lax.dot_general(
                sb_mixed, sb_out_w, (((0,), (0,)), ((), ())), preferred_element_type=jnp.float32
            )
            + jnp.einsum(
                "xnd,xdm->nm",
                delta_mixed,
                delta_out_w.reshape(fs_count, GDN_DIM, -1),
                preferred_element_type=jnp.float32,
            )
        ).astype(jnp.bfloat16),
        "tp",
        0,
    )
    return result.astype(jnp.bfloat16).reshape(1, result.shape[0], result.shape[1])


def solution(mesh):
    finer = Mesh(
        mesh.devices.reshape(8, 4, mesh.shape["fs"], mesh.shape["tp"]), ("sp_0", "sp_1", "fs", "tp")
    )
    return jax.shard_map(
        on_device,
        mesh=finer,
        in_specs=(
            P("fs", SP, "tp"),
            P("fs", "tp"),
            P("fs", "tp"),
            P("fs", "tp"),
            P("tp"),
            P("fs", "tp"),
            P("fs", "tp"),
            P("fs", "tp"),
            P(None, "tp"),
            P(None, "tp"),
            P("tp"),
            P("tp"),
            P("fs", "tp", SP),
            P(),
            P("tp", None),
            P("tp", None),
        ),
        out_specs=P("fs", SP_TP, None),
        check_vma=False,
    )
```

```python
import jax
import jax.numpy as jnp
from jax import lax
from jax.sharding import Mesh
from jax.experimental import pallas as pl
from jax.experimental.pallas import tpu as pltpu
from jax.sharding import PartitionSpec as P

SB_DIM = 64
GDN_DIM = 128
BLOCK = 64
SP = ("sp_0", "sp_1")
SP_TP = ("sp_0", "sp_1", "tp")


NORM_EPS = 1e-06


def joined_along(tiles, dim):
    tiles = jnp.moveaxis(tiles, 0, dim)
    shape = tiles.shape
    return tiles.reshape(*shape[:dim], shape[dim] * shape[dim + 1], *shape[dim + 2 :])


def sent_to_all(value, axis):
    devices = lax.axis_size(axis)
    return lax.all_to_all(
        jnp.broadcast_to(value[None], (devices, *value.shape)), axis, 0, 0, tiled=True
    )


def gathered_copies(value, axis, dim):
    return joined_along(sent_to_all(value, axis), dim)


def in_one_piece(arrays, axis, dim, along):
    widths = [a.shape[along] for a in arrays]
    both = jnp.concatenate(arrays, axis=along)
    result = lax.all_gather(both, axis, axis=dim, tiled=True)
    return tuple(jnp.split(result, [sum(widths[:k]) for k in range(1, len(widths))], axis=along))


def neutral_like(value, identity):
    return jax.tree.map(
        lambda part, zero: jnp.zeros_like(part) + jnp.asarray(zero, part.dtype), value, identity
    )


def entering(value, axes, combine, identity):
    before = start = neutral_like(value, identity)
    so_far = value
    for axis in reversed(axes):
        devices, index = (lax.axis_size(axis), lax.axis_index(axis))
        pieces = jax.tree.map(
            lambda part, kind: lax.all_gather(part.astype(kind), axis),
            so_far,
            (jnp.bfloat16, jnp.bfloat16),
        )
        inside, so_far = (start, start)
        for k in range(devices):
            passed = k < index
            so_far = combine(
                so_far, jax.tree.map(lambda part, own: part[k].astype(own.dtype), pieces, value)
            )
            inside = jax.tree.map(lambda new, old: jnp.where(passed, new, old), so_far, inside)
        before = combine(inside, before)
    return before


def split_up(value, dim, devices):
    before, after = (value.shape[:dim], value.shape[dim + 1 :])
    return jnp.moveaxis(value.reshape(*before, devices, -1, *after), dim, 0)


def sent_and_summed(value, axis, dim):
    tiles = split_up(value, dim, lax.axis_size(axis))
    arrived = lax.all_to_all(tiles, axis, split_axis=0, concat_axis=0, tiled=True)
    return arrived.astype(jnp.float32).sum(axis=0)


def unit_lower_inverse(strict_part):
    order_size = strict_part.shape[-1]
    powered = strict_part
    inverse = jnp.eye(order_size, dtype=strict_part.dtype) - strict_part
    for repeat_number in range(max(1, (order_size - 1).bit_length()) - 1):
        powered = jnp.einsum("...ij,...jk->...ik", powered, powered)
        inverse = inverse + jnp.einsum("...ij,...jk->...ik", inverse, powered)
    return inverse


def to_blocks(row_data, block_span):
    blocks_count = row_data.shape[0] // block_span
    shaped = row_data.reshape((blocks_count, block_span) + row_data.shape[1:])
    return jnp.swapaxes(shaped, 1, 2)


def from_blocks(blocked):
    swapped = jnp.swapaxes(blocked, 1, 2)
    return swapped.reshape((-1,) + swapped.shape[2:])


def unit_rows(vectors):
    return vectors * lax.rsqrt(jnp.sum(vectors * vectors, axis=-1, keepdims=True) + NORM_EPS)


def delta_inputs(
    query_proj,
    key_proj,
    value_proj,
    decay_pre,
    write_pre,
    write_bias,
    decay_log_scale,
    shift_rows,
    head_count,
    head_size,
):
    query_act = jax.nn.silu(query_proj.astype(jnp.float32)).reshape(-1, head_count, head_size)
    key_act = jax.nn.silu(key_proj.astype(jnp.float32)).reshape(-1, head_count, head_size)
    value_rows = jax.nn.silu(value_proj.astype(jnp.float32)).reshape(-1, head_count, head_size)
    queries = unit_rows(query_act) * head_size ** (-0.5)
    key_rows = unit_rows(key_act)
    log_decay = -jnp.exp(decay_log_scale) * jax.nn.softplus(decay_pre) + shift_rows
    strength = jax.nn.sigmoid(write_pre + write_bias)
    return (queries, key_rows, value_rows, log_decay, strength)


def delta_prepare(queries, key_rows, value_rows, log_decay, strength):
    block_span = queries.shape[2]
    cumulative = jnp.cumsum(log_decay, axis=-1)
    row_place = lax.broadcasted_iota(jnp.int32, (block_span, block_span), 0)
    col_place = lax.broadcasted_iota(jnp.int32, (block_span, block_span), 1)
    inclusive = col_place <= row_place
    strictly = col_place < row_place
    spread = cumulative[..., :, None] - cumulative[..., None, :]
    decay_table = jnp.where(inclusive, jnp.exp(jnp.where(inclusive, spread, 0.0)), 0.0)
    keys_beta = key_rows * strength[..., None]
    lower_part = jnp.where(
        strictly, jnp.einsum("nhik,nhjk->nhij", keys_beta, key_rows) * decay_table, 0.0
    )
    inverse = unit_lower_inverse(lower_part)
    growth = jnp.exp(cumulative)
    state_updates = jnp.einsum("nhij,nhjv->nhiv", inverse, value_rows * strength[..., None])
    erase_term = jnp.einsum("nhij,nhjk->nhik", inverse, keys_beta * growth[..., None])
    inside_block = jnp.einsum("nhik,nhjk->nhij", queries, key_rows) * decay_table
    boosted_query = queries * growth[..., None]
    damped_keys = key_rows * jnp.exp(cumulative[..., -1:] - cumulative)[..., None]
    decay_per_block = jnp.exp(cumulative[..., -1])
    return (state_updates, erase_term, inside_block, boosted_query, damped_keys, decay_per_block)


def delta_step(memory_state, inputs):
    state_updates, erase_term, inside_block, boosted_query, damped_keys, decay_per_block = inputs
    fixed_values = state_updates - jnp.einsum("mzq,mqc->mzc", erase_term, memory_state)
    produced_rows = jnp.einsum("mzq,mqc->mzc", boosted_query, memory_state) + jnp.einsum(
        "efq,eqn->efn", inside_block, fixed_values
    )
    memory_state = memory_state * decay_per_block[:, None, None] + jnp.einsum(
        "wam,waz->wmz", damped_keys, fixed_values
    )
    return (memory_state, produced_rows)


def transition_step(carried, inputs):
    memory_state, transfer = carried
    state_updates, erase_term, inside_block, boosted_query, damped_keys, decay_per_block = inputs
    fixed_values = state_updates - jnp.einsum("mzq,mqc->mzc", erase_term, memory_state)
    coupling = jnp.einsum("hik,hil->hkl", damped_keys, erase_term)
    memory_state = memory_state * decay_per_block[:, None, None] + jnp.einsum(
        "wam,waz->wmz", damped_keys, fixed_values
    )
    transfer = transfer * decay_per_block[:, None, None] - jnp.einsum(
        "hkl,hlm->hkm", coupling, transfer
    )
    return ((memory_state, transfer), None)


def compose(prior_blocks, following_blocks):
    joined_map = jnp.einsum("hkl,hlm->hkm", following_blocks[0], prior_blocks[0])
    joined_state = (
        jnp.einsum("djo,dog->djg", following_blocks[0], prior_blocks[1]) + following_blocks[1]
    )
    return (joined_map, joined_state)


def stick_kernel(offset_ref, query_ref, kv_ref, out_ref, later_ref, rows_ref, acc_ref, beyond_ref):
    place = lax.axis_index("sp_1")
    tile = query_ref.shape[2]
    size = query_ref.shape[1]
    groups = kv_ref.shape[2] // tile
    row_at = lax.broadcasted_iota(jnp.int32, (tile, tile), 0)
    col_at = lax.broadcasted_iota(jnp.int32, (tile, tile), 1)
    later_ref[...] = jnp.where(row_at > col_at, 1.0, 0.0).astype(jnp.bfloat16)
    offset = offset_ref[0]

    def key_row(row, blocks, diagonal):
        queries = rows_ref[...]
        beyond = None if diagonal else beyond_ref[...]
        weights = []
        for k in range(blocks - 1, -1, -1):
            scores = (
                jnp.dot(
                    queries,
                    kv_ref[row, 0:size, k * tile : (k + 1) * tile],
                    preferred_element_type=jnp.float32,
                )
                + offset
            )
            above = jnp.maximum(scores, 0.0)
            below = scores - above
            small = jnp.exp(below - above)
            log_term = jnp.where(small < 2.0**-12, small, jnp.log(1.0 + small))
            passed = above + log_term
            exponent = below - log_term
            if diagonal and k == blocks - 1:
                visible = col_at < row_at
                passed = jnp.where(visible, passed, 0.0)
                exponent = jnp.where(visible, exponent, -jnp.inf)
            after = jnp.dot(
                passed.astype(jnp.bfloat16), later_ref[...], preferred_element_type=jnp.float32
            )
            exponent = exponent - after
            if beyond is not None:
                exponent = exponent - beyond
            total = after[:, :1] + passed[:, :1]
            beyond = total if beyond is None else beyond + total
            weights.append(jnp.exp(exponent).astype(jnp.bfloat16))
        partial = lax.dot_general(
            jnp.concatenate(weights[::-1], axis=1),
            kv_ref[row, size : 2 * size, 0 : blocks * tile],
            (((1,), (1,)), ((), ())),
            preferred_element_type=jnp.float32,
        )
        beyond_ref[...] = beyond
        if diagonal:
            acc_ref[...] = partial
        else:
            acc_ref[...] += partial

    def per_query(query_row, unused):
        rows_ref[...] = (
            (query_ref[query_row].astype(jnp.float32) * size ** (-0.5)).T.astype(jnp.bfloat16)
        )
        for k in range(groups):

            @pl.when(place == k)
            def _():
                key_row(query_row, k + 1, True)

        def earlier(step, carried):
            key_row(query_row - 1 - step, groups, False)
            return carried

        lax.fori_loop(0, query_row, earlier, 0)
        out_ref[query_row] = acc_ref[...].T.astype(jnp.bfloat16)
        return unused

    lax.fori_loop(0, query_ref.shape[0], per_query, 0)


def stick_attention(offset, queries, keys_values):
    rows, size, tile = queries.shape
    return pl.pallas_call(
        stick_kernel,
        out_shape=jax.ShapeDtypeStruct((rows, size, tile), jnp.bfloat16),
        in_specs=[
            pl.BlockSpec(memory_space=pltpu.SMEM),
            pl.BlockSpec(memory_space=pltpu.VMEM),
            pl.BlockSpec(memory_space=pltpu.VMEM),
        ],
        out_specs=pl.BlockSpec(memory_space=pltpu.VMEM),
        scratch_shapes=[
            pltpu.VMEM((tile, tile), jnp.bfloat16),
            pltpu.VMEM((tile, size), jnp.bfloat16),
            pltpu.VMEM((tile, size), jnp.float32),
            pltpu.VMEM((tile, 1), jnp.float32),
        ],
        name="stick",
        cost_estimate=pl.CostEstimate(
            flops=40_000_000_000, bytes_accessed=3_000_000, transcendentals=27_000_000
        ),
    )(offset, queries, keys_values)

class Links:
    def __init__(self, send, recv):
        self.send, self.recv, self.count, self.sent, self.open = send, recv, 0, 0, []

    def number(self, n=1):
        self.count += n
        return self.count - n

    def copy(self, src, dst, k, axis, to):
        return pltpu.make_async_remote_copy(
            src_ref=src,
            dst_ref=dst,
            send_sem=self.send.at[self.sent],
            recv_sem=self.recv.at[k],
            device_id={axis: to},
            device_id_type=pl.DeviceIdType.MESH,
        )

    def start(self, src, dst, k, axis, to):
        made = self.copy(src, dst, k, axis, to)
        made.start()
        self.sent += 1
        self.open.append(made)

    def arrived(self, dst, k, axis):
        self.copy(dst, dst, k, axis, lax.axis_index(axis)).wait_recv()

    def drain(self):
        for made in self.open:
            made.wait_send()
        self.open = []


def greet(peers):
    barrier = pltpu.get_barrier_semaphore()
    for axis, to in peers:
        pl.semaphore_signal(
            barrier, inc=1, device_id={axis: to}, device_id_type=pl.DeviceIdType.MESH
        )
    pl.semaphore_wait(barrier, len(peers))


def project_kernel(
    hidden_ref, gates_ref, q0, k0, v0, q1, k1, v1,
    query_ref, kv_ref, delta_ref, pre_ref,
    acts, sb_w, delta_w, units, send, recv, local,
):
    z, y, x, t = (lax.axis_index(a) for a in ("sp_0", "sp_1", "fs", "tp"))
    nz, ny, nx = (lax.axis_size(a) for a in ("sp_0", "sp_1", "fs"))
    links = Links(send, recv)
    tokens = hidden_ref.shape[0]
    half = tokens // 2
    lanes = q0.shape[1] // nx
    z_rows, y_rows = q0.shape[0] // nz, q0.shape[0] // ny

    def at(axis, size, by):
        return lax.rem(lax.axis_index(axis) + by + size, size)

    greet(
        [("fs", at("fs", nx, d)) for d in range(1, nx)]
        + [("sp_0", at("sp_0", nz, d)) for d in range(1, nz)]
        + [("sp_1", at("sp_1", ny, d)) for d in (1, -1)]
        + [("tp", 1 - t)]
    )
    sets = ((q0, k0, v0), sb_w, z * z_rows, z_rows), ((q1, k1, v1), delta_w, y * y_rows, y_rows)
    width = 3 * lanes
    first = {}
    for d in (2, 1, 3):
        to = at("fs", nx, d)
        for s, (mats, held, row, size) in enumerate(sets):
            first[d, s] = links.number()
            for m, w in enumerate(mats):
                links.start(
                    w.at[pl.ds(row, size), pl.ds(to * lanes, lanes)],
                    held.at[x, pl.ds(row, size), m * lanes : (m + 1) * lanes],
                    first[d, s], "fs", to,
                )
    own = []
    for s, (mats, held, row, size) in enumerate(sets):
        for m, w in enumerate(mats):
            own.append(
                pltpu.make_async_copy(
                    w.at[pl.ds(row, size), pl.ds(x * lanes, lanes)],
                    held.at[x, pl.ds(row, size), m * lanes : (m + 1) * lanes],
                    local.at[3 * s + m],
                )
            )
            own[-1].start()
    right, left, other = at("fs", nx, 1), at("fs", nx, -1), 1 - t
    act = links.number(8)
    links.start(hidden_ref, acts.at[x, t], act, "fs", right)
    links.start(hidden_ref, acts.at[x, t], act + 1, "fs", left)
    links.start(hidden_ref, acts.at[x, t], act + 4, "tp", other)
    keep = pltpu.make_async_copy(hidden_ref, acts.at[x, t], local.at[6])
    keep.start()
    for made in own:
        made.wait()
    for d in (1, 3, 2):
        source = at("fs", nx, -d)
        for s, (mats, held, row, size) in enumerate(sets):
            links.arrived(held.at[source, pl.ds(row, size), 0:width], first[d, s], "fs")

    def sb_piece(by, low=0, count=nx):
        return sb_w.at[low : low + count, pl.ds(at("sp_0", nz, by) * z_rows, z_rows), :]

    def delta_piece(by, low=0, count=nx):
        rows = pl.ds(at("sp_1", ny, by) * y_rows, y_rows)
        return delta_w.at[low : low + count, rows, 0:width]

    z_right, z_left = at("sp_0", nz, 1), at("sp_0", nz, -1)
    y_right, y_left = at("sp_1", ny, 1), at("sp_1", ny, -1)
    steps = nz // 2
    zr, zl = links.number(steps), links.number(steps)
    yr, yl = links.number(2), links.number(2)
    links.start(sb_piece(0), sb_piece(0), zr, "sp_0", z_right)
    links.start(sb_piece(0), sb_piece(0), zl, "sp_0", z_left)
    links.start(delta_piece(0), delta_piece(0), yr, "sp_1", y_right)
    links.start(delta_piece(0), delta_piece(0), yl, "sp_1", y_left)

    def z_step(s):
        if s < steps:
            low, count = (0, nx) if s < steps - 1 else (0, nx // 2)
            links.arrived(sb_piece(-s), zr + s - 1, "sp_0")
            links.start(sb_piece(-s, low, count), sb_piece(-s, low, count), zr + s, "sp_0", z_right)
            low, count = (0, nx) if s < steps - 1 else (nx // 2, nx // 2)
            links.arrived(sb_piece(s), zl + s - 1, "sp_0")
            links.start(sb_piece(s, low, count), sb_piece(s, low, count), zl + s, "sp_0", z_left)
        else:
            links.arrived(sb_piece(steps, 0, nx // 2), zr + s - 1, "sp_0")
            links.arrived(sb_piece(steps, nx // 2, nx // 2), zl + s - 1, "sp_0")

    z_step(1)
    links.arrived(delta_piece(-1), yr, "sp_1")
    links.start(delta_piece(-1, 0, 2), delta_piece(-1, 0, 2), yr + 1, "sp_1", y_right)
    links.arrived(delta_piece(1), yl, "sp_1")
    links.start(delta_piece(1, 2, 2), delta_piece(1, 2, 2), yl + 1, "sp_1", y_left)
    z_step(2)
    before, after, far = at("fs", nx, -1), at("fs", nx, 1), at("fs", nx, 2)
    links.arrived(acts.at[before, t], act, "fs")
    links.start(acts.at[before, t, 0:half], acts.at[before, t, 0:half], act + 2, "fs", right)
    links.start(acts.at[before, t], acts.at[before, t], act + 5, "tp", other)
    links.arrived(acts.at[after, t], act + 1, "fs")
    links.start(
        acts.at[after, t, half:tokens], acts.at[after, t, half:tokens], act + 3, "fs", left
    )
    links.start(acts.at[after, t], acts.at[after, t], act + 6, "tp", other)
    z_step(3)
    delta_w[:, :, width : width + lanes] = gates_ref[...]
    z_step(4)
    links.arrived(delta_piece(2, 0, 2), yr + 1, "sp_1")
    links.arrived(delta_piece(2, 2, 2), yl + 1, "sp_1")
    links.arrived(acts.at[far, t, 0:half], act + 2, "fs")
    links.arrived(acts.at[far, t, half:tokens], act + 3, "fs")
    links.start(acts.at[far, t], acts.at[far, t], act + 7, "tp", other)
    keep.wait()
    for k, c in enumerate((x, before, after, far)):
        links.arrived(acts.at[c, other], act + 4 + k, "tp")

    size = lanes // 2
    zq, zk = links.number(nz), links.number(nz)

    def product(c, held, cols):
        return sum(
            jnp.dot(
                acts[c, p],
                held[2 * p : 2 * p + 2, :, cols].reshape(acts.shape[3], -1),
                preferred_element_type=jnp.float32,
            )
            for p in range(2)
        )

    def sb_sequence(c, carried):
        for m in range(3):
            block = product(c, sb_w, slice(m * lanes, (m + 1) * lanes)).T.astype(jnp.bfloat16)
            units[2 * c, m * size : (m + 1) * size, :] = block[0:size]
            units[2 * c + 1, m * size : (m + 1) * size, :] = block[size:lanes]
        return carried

    lax.fori_loop(0, nx, sb_sequence, 0)

    def delta_sequence(c, carried):
        out = product(c, delta_w, slice(0, width + lanes))
        delta_ref[c] = out[:, 0:width].astype(jnp.bfloat16)
        pre_ref[c] = out[:, width : width + lanes]
        return carried

    delta_sequence(0, 0)

    here = pl.ds(pl.multiple_of(y * tokens, tokens), tokens)
    for d in (4, 3, 5, 2, 6, 1, 7):
        to = at("sp_0", nz, d)
        links.start(units.at[to, 0:size], query_ref.at[z], zq + d, "sp_0", to)
        links.start(units.at[to, size : 3 * size], kv_ref.at[z, :, here], zk + d, "sp_0", to)
    mine = (
        pltpu.make_async_copy(units.at[z, 0:size], query_ref.at[z], local.at[7]),
        pltpu.make_async_copy(units.at[z, size : 3 * size], kv_ref.at[z, :, here], local.at[8]),
    )
    for made in mine:
        made.start()
    lax.fori_loop(1, nx, delta_sequence, 0)
    for made in mine:
        made.wait()
    kv_r, kv_l = links.number(nz), links.number(nz)
    kv_rr, kv_ll = links.number(nz), links.number(nz)
    order = (0, 1, 7, 2, 6, 3, 5, 4)

    def kv_piece(row, by, low=0, count=2 * size):
        cols = pl.ds(pl.multiple_of(at("sp_1", ny, by) * tokens, tokens), tokens)
        return kv_ref.at[row, low : low + count, cols]

    def forward(d):
        row = at("sp_0", nz, -d)
        links.arrived(kv_piece(row, -1), kv_r + d, "sp_1")
        links.start(
            kv_piece(row, -1, 0, size), kv_piece(row, -1, 0, size), kv_rr + d, "sp_1", y_right
        )
        links.arrived(kv_piece(row, 1), kv_l + d, "sp_1")
        links.start(
            kv_piece(row, 1, size, size), kv_piece(row, 1, size, size), kv_ll + d, "sp_1", y_left
        )

    for i, d in enumerate(order):
        row = at("sp_0", nz, -d)
        if d:
            links.arrived(kv_ref.at[row, :, here], zk + d, "sp_0")
        links.start(kv_piece(row, 0), kv_piece(row, 0), kv_r + d, "sp_1", y_right)
        links.start(kv_piece(row, 0), kv_piece(row, 0), kv_l + d, "sp_1", y_left)
        if i >= 2:
            forward(order[i - 2])
    for d in order[-2:]:
        forward(d)
    for d in order:
        row = at("sp_0", nz, -d)
        if d:
            links.arrived(query_ref.at[row], zq + d, "sp_0")
        links.arrived(kv_piece(row, 2, 0, size), kv_rr + d, "sp_1")
        links.arrived(kv_piece(row, 2, size, size), kv_ll + d, "sp_1")
    links.drain()


def project_and_share(hidden, gates, sb_weights, delta_weights):
    nz, ny, nx = (lax.axis_size(a) for a in ("sp_0", "sp_1", "fs"))
    tokens, part = hidden.shape
    rows, lanes = sb_weights[0].shape[0], sb_weights[0].shape[1] // nx
    size = lanes // 2
    vmem = pl.BlockSpec(memory_space=pltpu.VMEM)
    anywhere = pl.BlockSpec(memory_space=pl.ANY)
    copies = 96
    return pl.pallas_call(
        project_kernel,
        out_shape=(
            jax.ShapeDtypeStruct((nz, size, tokens), jnp.bfloat16),
            jax.ShapeDtypeStruct((nz, 2 * size, ny * tokens), jnp.bfloat16),
            jax.ShapeDtypeStruct((nx, tokens, 3 * lanes), jnp.bfloat16),
            jax.ShapeDtypeStruct((nx, tokens, lanes), jnp.float32),
        ),
        in_specs=[vmem, vmem] + [anywhere] * 6,
        out_specs=(vmem,) * 4,
        scratch_shapes=[
            pltpu.VMEM((nx, 2, tokens, part), jnp.bfloat16),
            pltpu.VMEM((nx, rows, 3 * lanes), jnp.bfloat16),
            pltpu.VMEM((nx, rows, 4 * lanes), jnp.bfloat16),
            pltpu.VMEM((nz, 3 * size, tokens), jnp.bfloat16),
            pltpu.SemaphoreType.DMA((copies,)),
            pltpu.SemaphoreType.DMA((copies,)),
            pltpu.SemaphoreType.DMA((9,)),
        ],
        compiler_params=pltpu.CompilerParams(collective_id=0, has_side_effects=True),
        name="project",
        cost_estimate=pl.CostEstimate(
            flops=60_000_000_000, bytes_accessed=10_000_000, transcendentals=0
        ),
    )(hidden, gates, *sb_weights, *delta_weights)


def on_device(
    hidden_in,
    sb_query_w,
    sb_key_w,
    sb_value_w,
    sb_offset,
    delta_query_w,
    delta_key_w,
    delta_value_w,
    decay_w,
    write_w,
    write_bias,
    decay_log_scale,
    decay_shift,
    head_gain,
    sb_out_w,
    delta_out_w,
):
    tokens, part = hidden_in.shape[1], hidden_in.shape[2]
    fs_count = lax.axis_size("fs")
    mine = lax.axis_index("fs")
    gates_w = jnp.concatenate(
        [lax.dynamic_slice_in_dim(w, mine, 1, 1) for w in (decay_w, write_w)], axis=1
    )
    lanes = sb_query_w.shape[1] // fs_count
    gates_w = jnp.pad(gates_w, ((0, 0), (0, lanes - 2))).reshape(fs_count, -1, lanes)
    head_pair = sb_offset.shape[0] // fs_count
    unit_queries, keys_values, delta_proj, gates = project_and_share(
        hidden_in.reshape(tokens, part),
        gates_w,
        (sb_query_w, sb_key_w, sb_value_w),
        (delta_query_w, delta_key_w, delta_value_w),
    )
    offset = lax.dynamic_slice_in_dim(
        sb_offset, head_pair * mine + lax.rem(lax.axis_index("sp_0"), head_pair), 1, 0
    )
    sb_out = stick_attention(offset, unit_queries, keys_values)
    dq, dk, dv = (
        delta_proj[:, :, k * GDN_DIM : (k + 1) * GDN_DIM]
        .transpose(1, 0, 2)
        .reshape(tokens, fs_count * GDN_DIM)
        for k in range(3)
    )
    shift_rows = lax.all_to_all(
        decay_shift.reshape(decay_log_scale.shape[0], tokens), "fs", 0, 0, tiled=True
    ).T
    own_bias = jnp.broadcast_to(lax.dynamic_slice_in_dim(write_bias, mine, 1, 0), (fs_count,))
    own_scale = jnp.broadcast_to(
        lax.dynamic_slice_in_dim(decay_log_scale, mine, 1, 0), (fs_count,)
    )
    queries, key_rows, value_rows, log_decay, strength = delta_inputs(
        dq, dk, dv, gates[:, :, 0].T, gates[:, :, 1].T, own_bias, own_scale, shift_rows, fs_count, GDN_DIM
    )
    prepared = delta_prepare(
        to_blocks(queries, BLOCK),
        to_blocks(key_rows, BLOCK),
        to_blocks(value_rows, BLOCK),
        to_blocks(log_decay, BLOCK),
        to_blocks(strength, BLOCK),
    )
    identity_map = jnp.broadcast_to(
        jnp.eye(GDN_DIM, dtype=jnp.float32), (fs_count, GDN_DIM, GDN_DIM)
    )
    empty_state = jnp.zeros((fs_count, GDN_DIM, GDN_DIM), jnp.float32)
    (local_end, local_map), unused_out = lax.scan(
        transition_step, (empty_state, identity_map), prepared
    )
    unused_map, incoming = entering(
        (local_map, local_end), SP, compose, (identity_map, empty_state)
    )
    unused_end, produced_rows = lax.scan(delta_step, incoming, prepared)
    produced_rows = from_blocks(produced_rows)
    normed = (
        produced_rows
        * lax.rsqrt(jnp.mean(produced_rows * produced_rows, axis=-1, keepdims=True) + NORM_EPS)
        * head_gain
    )
    delta_mixed = lax.all_to_all(
        normed.astype(jnp.bfloat16).transpose(1, 0, 2), "fs", 0, 0, tiled=True
    )
    sb_back = lax.all_to_all(sb_out, "sp_0", 0, 0, tiled=True)
    sb_mixed = lax.all_to_all(
        sb_back.reshape(fs_count, head_pair * SB_DIM, tokens), "fs", 0, 0, tiled=True
    ).reshape(-1, tokens)
    result = sent_and_summed(
        (
            lax.dot_general(
                sb_mixed, sb_out_w, (((0,), (0,)), ((), ())), preferred_element_type=jnp.float32
            )
            + jnp.einsum(
                "xnd,xdm->nm",
                delta_mixed,
                delta_out_w.reshape(fs_count, GDN_DIM, -1),
                preferred_element_type=jnp.float32,
            )
        ).astype(jnp.bfloat16),
        "tp",
        0,
    )
    return result.astype(jnp.bfloat16).reshape(1, result.shape[0], result.shape[1])


def solution(mesh):
    finer = Mesh(
        mesh.devices.reshape(8, 4, mesh.shape["fs"], mesh.shape["tp"]), ("sp_0", "sp_1", "fs", "tp")
    )
    return jax.shard_map(
        on_device,
        mesh=finer,
        in_specs=(
            P("fs", SP, "tp"),
            P("fs", "tp"),
            P("fs", "tp"),
            P("fs", "tp"),
            P("tp"),
            P("fs", "tp"),
            P("fs", "tp"),
            P("fs", "tp"),
            P(None, "tp"),
            P(None, "tp"),
            P("tp"),
            P("tp"),
            P("fs", "tp", SP),
            P(),
            P("tp", None),
            P("tp", None),
        ),
        out_specs=P("fs", SP_TP, None),
        check_vma=False,
    )
```

```python
import jax
import jax.numpy as jnp
from jax import lax
from jax.experimental import pallas as pl
from jax.experimental.pallas import tpu as pltpu
from jax.sharding import Mesh
from jax.sharding import PartitionSpec as P

SB_DIM = 64
GDN_DIM = 128
BLOCK = 64
SP = ("sp_0", "sp_1")
SP_TP = ("sp_0", "sp_1", "tp")
NORM_EPS = 1e-06


def unit_rows(vectors):
    return vectors * lax.rsqrt(jnp.sum(vectors * vectors, axis=-1, keepdims=True) + NORM_EPS)


class Links:
    def __init__(self, send, recv, me):
        self.me = me
        self.send, self.recv, self.count, self.sent, self.open = send, recv, 0, 0, []

    def number(self, n=1):
        self.count += n
        return self.count - n

    def copy(self, src, dst, k, axis, to):
        return pltpu.make_async_remote_copy(
            src_ref=src,
            dst_ref=dst,
            send_sem=self.send.at[self.sent],
            recv_sem=self.recv.at[k],
            device_id={axis: to},
            device_id_type=pl.DeviceIdType.MESH,
        )

    def start(self, src, dst, k, axis, to, like=None):
        made = self.copy(src, dst, k, axis, to)
        made.start()
        self.open.append((made, self.sent, like, axis))
        self.sent += 1

    def arrived(self, dst, k, axis):
        self.copy(dst, dst, k, axis, self.me[axis]).wait_recv()

    def drain(self):
        for made, sent, like, axis in self.open:
            if like is not None:
                self.sent = sent
                made = self.copy(like(), like(), 0, axis, self.me[axis])
            made.wait_send()
        self.open = []


def greet(peers):
    barrier = pltpu.get_barrier_semaphore()
    for axis, to in peers:
        pl.semaphore_signal(
            barrier, inc=1, device_id={axis: to}, device_id_type=pl.DeviceIdType.MESH
        )
    pl.semaphore_wait(barrier, len(peers))


def project_kernel(
    hidden_ref, gates_ref, shift_in, q0, k0, v0, q1, k1, v1,
    query_ref, kv_ref, delta_ref, pre_ref, shift_ref,
    acts, sb_w, delta_w, units, send, recv, local,
):
    z, y, x, t = (lax.axis_index(a) for a in ("sp_0", "sp_1", "fs", "tp"))
    nz, ny, nx = (lax.axis_size(a) for a in ("sp_0", "sp_1", "fs"))
    me = {"sp_0": z, "sp_1": y, "fs": x, "tp": t}
    links = Links(send, recv, me)
    tokens = hidden_ref.shape[0]
    half = tokens // 2
    lanes = q0.shape[1] // nx
    z_rows, y_rows = q0.shape[0] // nz, q0.shape[0] // ny

    def at(axis, size, by):
        return lax.rem(me[axis] + by + size, size)

    greet(
        [("fs", at("fs", nx, d)) for d in range(1, nx)]
        + [("sp_0", at("sp_0", nz, d)) for d in range(1, nz)]
        + [("sp_1", at("sp_1", ny, d)) for d in (1, -1)]
        + [("tp", 1 - t)]
    )
    sets = ((q0, k0, v0), sb_w, z * z_rows, z_rows), ((q1, k1, v1), delta_w, y * y_rows, y_rows)
    width = 3 * lanes
    first = {}
    for d in (2, 1, 3):
        to = at("fs", nx, d)
        for s, (mats, held, row, size) in enumerate(sets):
            first[d, s] = links.number()
            for m, w in enumerate(mats):
                links.start(
                    w.at[pl.ds(row, size), pl.ds(to * lanes, lanes)],
                    held.at[x, pl.ds(row, size), m * lanes : (m + 1) * lanes],
                    first[d, s], "fs", to,
                )
    own = []
    for s, (mats, held, row, size) in enumerate(sets):
        for m, w in enumerate(mats):
            own.append(
                pltpu.make_async_copy(
                    w.at[pl.ds(row, size), pl.ds(x * lanes, lanes)],
                    held.at[x, pl.ds(row, size), m * lanes : (m + 1) * lanes],
                    local.at[3 * s + m],
                )
            )
            own[-1].start()
    shifts = links.number(nx)
    for d in range(1, nx):
        links.start(shift_in.at[at("fs", nx, d)], shift_ref.at[x], shifts + d, "fs", at("fs", nx, d))
    own.append(pltpu.make_async_copy(shift_in.at[x], shift_ref.at[x], local.at[9]))
    own[-1].start()
    right, left, other = at("fs", nx, 1), at("fs", nx, -1), 1 - t
    act = links.number(8)
    links.start(hidden_ref, acts.at[x, t], act, "fs", right)
    links.start(hidden_ref, acts.at[x, t], act + 1, "fs", left)
    links.start(hidden_ref, acts.at[x, t], act + 4, "tp", other)
    keep = pltpu.make_async_copy(hidden_ref, acts.at[x, t], local.at[6])
    keep.start()
    for made in own:
        made.wait()
    for d in (1, 3, 2):
        source = at("fs", nx, -d)
        for s, (mats, held, row, size) in enumerate(sets):
            links.arrived(held.at[source, pl.ds(row, size), 0:width], first[d, s], "fs")

    def sb_piece(by, low=0, count=nx):
        return sb_w.at[low : low + count, pl.ds(at("sp_0", nz, by) * z_rows, z_rows), :]

    def delta_piece(by, low=0, count=nx):
        rows = pl.ds(at("sp_1", ny, by) * y_rows, y_rows)
        return delta_w.at[low : low + count, rows, 0:width]

    z_right, z_left = at("sp_0", nz, 1), at("sp_0", nz, -1)
    y_right, y_left = at("sp_1", ny, 1), at("sp_1", ny, -1)
    steps = nz // 2
    zr, zl = links.number(steps), links.number(steps)
    yr, yl = links.number(2), links.number(2)
    links.start(sb_piece(0), sb_piece(0), zr, "sp_0", z_right)
    links.start(sb_piece(0), sb_piece(0), zl, "sp_0", z_left)
    links.start(delta_piece(0), delta_piece(0), yr, "sp_1", y_right)
    links.start(delta_piece(0), delta_piece(0), yl, "sp_1", y_left)

    def z_step(s):
        if s < steps:
            low, count = (0, nx) if s < steps - 1 else (0, nx // 2)
            links.arrived(sb_piece(-s), zr + s - 1, "sp_0")
            links.start(sb_piece(-s, low, count), sb_piece(-s, low, count), zr + s, "sp_0", z_right)
            low, count = (0, nx) if s < steps - 1 else (nx // 2, nx // 2)
            links.arrived(sb_piece(s), zl + s - 1, "sp_0")
            links.start(sb_piece(s, low, count), sb_piece(s, low, count), zl + s, "sp_0", z_left)
        else:
            links.arrived(sb_piece(steps, 0, nx // 2), zr + s - 1, "sp_0")
            links.arrived(sb_piece(steps, nx // 2, nx // 2), zl + s - 1, "sp_0")

    z_step(1)
    links.arrived(delta_piece(-1), yr, "sp_1")
    links.start(delta_piece(-1, 0, 2), delta_piece(-1, 0, 2), yr + 1, "sp_1", y_right)
    links.arrived(delta_piece(1), yl, "sp_1")
    links.start(delta_piece(1, 2, 2), delta_piece(1, 2, 2), yl + 1, "sp_1", y_left)
    z_step(2)
    before, after, far = at("fs", nx, -1), at("fs", nx, 1), at("fs", nx, 2)
    links.arrived(acts.at[before, t], act, "fs")
    links.start(acts.at[before, t, 0:half], acts.at[before, t, 0:half], act + 2, "fs", right)
    links.start(acts.at[before, t], acts.at[before, t], act + 5, "tp", other)
    links.arrived(acts.at[after, t], act + 1, "fs")
    links.start(
        acts.at[after, t, half:tokens], acts.at[after, t, half:tokens], act + 3, "fs", left
    )
    links.start(acts.at[after, t], acts.at[after, t], act + 6, "tp", other)
    z_step(3)
    delta_w[:, :, width : width + lanes] = gates_ref[...]
    z_step(4)
    links.arrived(delta_piece(2, 0, 2), yr + 1, "sp_1")
    links.arrived(delta_piece(2, 2, 2), yl + 1, "sp_1")
    links.arrived(acts.at[far, t, 0:half], act + 2, "fs")
    links.arrived(acts.at[far, t, half:tokens], act + 3, "fs")
    links.start(acts.at[far, t], acts.at[far, t], act + 7, "tp", other)
    keep.wait()
    for k, c in enumerate((x, before, after, far)):
        links.arrived(acts.at[c, other], act + 4 + k, "tp")

    size = lanes // 2
    zq, zk = links.number(nz), links.number(nz)

    def product(c, held, cols):
        return sum(
            jnp.dot(
                acts[c, p],
                held[2 * p : 2 * p + 2, :, cols].reshape(acts.shape[3], -1),
                preferred_element_type=jnp.float32,
            )
            for p in range(2)
        )

    def sb_sequence(c, carried):
        for m in range(3):
            block = product(c, sb_w, slice(m * lanes, (m + 1) * lanes)).T.astype(jnp.bfloat16)
            units[2 * c, m * size : (m + 1) * size, :] = block[0:size]
            units[2 * c + 1, m * size : (m + 1) * size, :] = block[size:lanes]
        return carried

    lax.fori_loop(0, nx, sb_sequence, 0)

    def delta_sequence(c, carried):
        out = product(c, delta_w, slice(0, width + lanes))
        delta_ref[c] = out[:, 0:width].astype(jnp.bfloat16)
        pre_ref[c] = out[:, width : width + lanes].T[0:8]
        return carried

    delta_sequence(0, 0)

    here = pl.ds(pl.multiple_of(y * tokens, tokens), tokens)
    for d in (4, 3, 5, 2, 6, 1, 7):
        to = at("sp_0", nz, d)
        links.start(units.at[to, 0:size], query_ref.at[z], zq + d, "sp_0", to)
        links.start(units.at[to, size : 3 * size], kv_ref.at[z, :, here], zk + d, "sp_0", to)
    mine = (
        pltpu.make_async_copy(units.at[z, 0:size], query_ref.at[z], local.at[7]),
        pltpu.make_async_copy(units.at[z, size : 3 * size], kv_ref.at[z, :, here], local.at[8]),
    )
    for made in mine:
        made.start()
    lax.fori_loop(1, nx, delta_sequence, 0)
    for made in mine:
        made.wait()
    kv_r, kv_l = links.number(nz), links.number(nz)
    kv_rr, kv_ll = links.number(nz), links.number(nz)
    order = (0, 1, 7, 2, 6, 3, 5, 4)

    def kv_piece(row, by, low=0, count=2 * size):
        cols = pl.ds(pl.multiple_of(at("sp_1", ny, by) * tokens, tokens), tokens)
        return kv_ref.at[row, low : low + count, cols]

    def forward(d):
        row = at("sp_0", nz, -d)
        links.arrived(kv_piece(row, -1), kv_r + d, "sp_1")
        links.start(
            kv_piece(row, -1, 0, size), kv_piece(row, -1, 0, size), kv_rr + d, "sp_1", y_right
        )
        links.arrived(kv_piece(row, 1), kv_l + d, "sp_1")
        links.start(
            kv_piece(row, 1, size, size), kv_piece(row, 1, size, size), kv_ll + d, "sp_1", y_left
        )

    for i, d in enumerate(order):
        row = at("sp_0", nz, -d)
        if d:
            links.arrived(kv_ref.at[row, :, here], zk + d, "sp_0")
        links.start(kv_piece(row, 0), kv_piece(row, 0), kv_r + d, "sp_1", y_right)
        links.start(kv_piece(row, 0), kv_piece(row, 0), kv_l + d, "sp_1", y_left)
        if i >= 2:
            forward(order[i - 2])
    for d in order[-2:]:
        forward(d)
    for d in order:
        row = at("sp_0", nz, -d)
        if d:
            links.arrived(query_ref.at[row], zq + d, "sp_0")
        links.arrived(kv_piece(row, 2, 0, size), kv_rr + d, "sp_1")
        links.arrived(kv_piece(row, 2, size, size), kv_ll + d, "sp_1")
    for d in range(1, nx):
        links.arrived(shift_ref.at[at("fs", nx, -d)], shifts + d, "fs")
    links.drain()


def project_and_share(hidden, gates, shift, sb_weights, delta_weights):
    nz, ny, nx = (lax.axis_size(a) for a in ("sp_0", "sp_1", "fs"))
    tokens, part = hidden.shape
    rows, lanes = sb_weights[0].shape[0], sb_weights[0].shape[1] // nx
    size = lanes // 2
    vmem = pl.BlockSpec(memory_space=pltpu.VMEM)
    anywhere = pl.BlockSpec(memory_space=pl.ANY)
    copies = 96
    return pl.pallas_call(
        project_kernel,
        out_shape=(
            jax.ShapeDtypeStruct((nz, size, tokens), jnp.bfloat16),
            jax.ShapeDtypeStruct((nz, 2 * size, ny * tokens), jnp.bfloat16),
            jax.ShapeDtypeStruct((nx, tokens, 3 * lanes), jnp.bfloat16),
            jax.ShapeDtypeStruct((nx, 8, tokens), jnp.float32),
            jax.ShapeDtypeStruct((nx, 1, tokens), jnp.float32),
        ),
        in_specs=[vmem] * 3 + [anywhere] * 6,
        out_specs=(vmem,) * 5,
        scratch_shapes=[
            pltpu.VMEM((nx, 2, tokens, part), jnp.bfloat16),
            pltpu.VMEM((nx, rows, 3 * lanes), jnp.bfloat16),
            pltpu.VMEM((nx, rows, 4 * lanes), jnp.bfloat16),
            pltpu.VMEM((nz, 3 * size, tokens), jnp.bfloat16),
            pltpu.SemaphoreType.DMA((copies,)),
            pltpu.SemaphoreType.DMA((copies,)),
            pltpu.SemaphoreType.DMA((10,)),
        ],
        compiler_params=pltpu.CompilerParams(collective_id=0, has_side_effects=True),
        name="project",
        cost_estimate=pl.CostEstimate(
            flops=60_000_000_000, bytes_accessed=10_000_000, transcendentals=0
        ),
    )(hidden, gates, shift, *sb_weights, *delta_weights)


def mix_kernel(
    offset_ref, bias_ref, scale_ref, query_ref, kv_ref, delta_ref, pre_ref, shift_ref, gain_ref,
    sb_out_ref, delta_out_ref,
    result_ref,
    later_ref, rows_ref, acc_ref, beyond_ref, done_ref, sb_in, delta_in, delta_done,
    through, local_out, transfer, stage1, stage2, leaving, incoming,
    sb_out_w, delta_out_w, given, taken, send, recv, local,
):
    z, y, x, t = (lax.axis_index(a) for a in ("sp_0", "sp_1", "fs", "tp"))
    nz, ny, nx = (lax.axis_size(a) for a in ("sp_0", "sp_1", "fs"))
    me = {"sp_0": z, "sp_1": y, "fs": x, "tp": t}
    links = Links(send, recv, me)
    tile, size = query_ref.shape[2], query_ref.shape[1]
    groups = kv_ref.shape[2] // tile
    key = delta_ref.shape[2] // 3

    def at(axis, count, by):
        return lax.rem(me[axis] + by + count, count)

    loads = [
        pltpu.make_async_copy(sb_out_ref, sb_out_w, local.at[0]),
        pltpu.make_async_copy(delta_out_ref, delta_out_w, local.at[1]),
    ]
    for made in loads:
        made.start()
    barrier = pltpu.get_barrier_semaphore()
    peers = [
        {"sp_0": at("sp_0", nz, dz), "fs": at("fs", nx, dx)}
        for dz in range(nz)
        for dx in range(nx)
        if dz or dx
    ]
    peers += [{"sp_1": at("sp_1", ny, d)} for d in range(1, ny)] + [{"tp": 1 - t}]
    for peer in peers:
        pl.semaphore_signal(barrier, inc=1, device_id=peer, device_id_type=pl.DeviceIdType.MESH)
    pl.semaphore_wait(barrier, len(peers))

    row_at = lax.broadcasted_iota(jnp.int32, (tile, tile), 0)
    col_at = lax.broadcasted_iota(jnp.int32, (tile, tile), 1)
    later_ref[...] = jnp.where(row_at > col_at, 1.0, 0.0).astype(jnp.bfloat16)
    offset = offset_ref[2 * x + lax.rem(z, 2)]

    def low(a):
        return a.astype(jnp.bfloat16)

    def mul(a, b, contract=((1,), (0,))):
        return lax.dot_general(
            low(a), low(b), (contract, ((), ())), preferred_element_type=jnp.float32
        )

    same = row_at // BLOCK == col_at // BLOCK
    inclusive = same & (col_at <= row_at)
    strictly = same & (col_at < row_at)
    decay_pre = jnp.concatenate([pre_ref[s, 0:1] for s in range(nx)], axis=0)
    write_pre = jnp.concatenate([pre_ref[s, 1:2] for s in range(nx)], axis=0)
    shift = jnp.concatenate([shift_ref[s] for s in range(nx)], axis=0)
    softplus = jnp.maximum(decay_pre, 0.0) + jnp.log1p(jnp.exp(-jnp.abs(decay_pre)))
    rate = jnp.exp(jnp.full(decay_pre.shape, scale_ref[x], jnp.float32))
    log_decay = shift - rate * softplus
    strength = jax.nn.sigmoid(write_pre + bias_ref[x])
    up_to = jnp.where(same & (row_at <= col_at), 1.0, 0.0)
    both = jnp.concatenate([log_decay, strength], axis=0)
    summed = jnp.dot(
        both, up_to, preferred_element_type=jnp.float32, precision=lax.Precision.HIGHEST
    )
    sums_col = summed.T
    both_col = both.T
    blocks = tile // BLOCK

    def local_part(s):
        cum_row = summed[s : s + 1]
        cum = sums_col[:, s : s + 1]
        beta = both_col[:, nx + s : nx + s + 1]
        act = jax.nn.silu(delta_ref[s].astype(jnp.float32))
        q, k, v = act[:, 0:key], act[:, key : 2 * key], act[:, 2 * key : 3 * key]
        q = unit_rows(q) * key ** (-0.5)
        k = unit_rows(k)
        spread = cum - cum_row
        decay = jnp.where(inclusive, jnp.exp(jnp.where(inclusive, spread, 0.0)), 0.0)
        k_beta = k * beta
        lower = jnp.where(strictly, mul(k_beta, k, ((1,), (1,))) * decay, 0.0)
        inside = mul(q, k, ((1,), (1,))) * decay
        powered = lower
        inverse = jnp.where(row_at == col_at, 1.0, 0.0) - lower
        for _ in range(max(1, (BLOCK - 1).bit_length()) - 1):
            powered = mul(powered, powered)
            inverse = inverse + mul(inverse, powered)
        growth = jnp.exp(cum)
        updates = mul(inverse, jnp.concatenate([v * beta, k_beta * growth], axis=1))
        within = mul(inside, updates)
        reach = q * growth - within[:, key:]
        last = [cum[(b + 1) * BLOCK - 1 : (b + 1) * BLOCK] for b in range(blocks)]
        carried = None
        eye = jnp.where(
            lax.broadcasted_iota(jnp.int32, (key, key), 0)
            == lax.broadcasted_iota(jnp.int32, (key, key), 1),
            1.0,
            0.0,
        )
        zero = jnp.zeros((key, key), jnp.float32)
        for b in range(blocks):
            rows = slice(b * BLOCK, (b + 1) * BLOCK)
            damped = k[rows] * jnp.exp(last[b] - cum[rows])
            step = mul(damped, updates[rows], ((0,), (0,)))
            keep = jnp.exp(last[b])
            start = jnp.concatenate([zero, eye], axis=1) if carried is None else carried
            out = mul(reach[rows], start)
            local_out[s, rows] = within[rows, 0:key] + out[:, 0:key]
            through[s, rows] = low(out[:, key:])
            carried = (
                start * keep
                - mul(step[:, key:], start)
                + jnp.concatenate([step[:, 0:key], zero], axis=1)
            )
        transfer[s] = low(carried)

    for s in range(nx):
        local_part(s)

    one = links.number(ny)
    for d in (2, 1, 3):
        to = at("sp_1", ny, d)
        links.start(transfer.at[to], stage1.at[y], one + d, "sp_1", to)
    mine = pltpu.make_async_copy(transfer.at[y], stage1.at[y], local.at[2])
    mine.start()
    two, three = links.number(nz), links.number(ny)
    keep_own = pltpu.make_async_copy(leaving.at[y], incoming.at[y], local.at[3])

    def over_group():
        mine.wait()
        for d in range(1, ny):
            links.arrived(stage1.at[at("sp_1", ny, -d)], one + d, "sp_1")
        joined = stage1[0].astype(jnp.float32)
        for k in range(1, ny):
            own = stage1[k]
            new = mul(own[:, key:], joined)
            joined = jnp.concatenate(
                [new[:, 0:key] + own[:, 0:key].astype(jnp.float32), new[:, key:]], axis=1
            )
        stage2[z] = low(joined)

    def share_group():
        for d in (4, 3, 5, 2, 6, 1, 7):
            links.start(stage2.at[z], stage2.at[z], two + d, "sp_0", at("sp_0", nz, d), lambda: stage2.at[0])

    def over_line():
        for d in range(1, nz):
            links.arrived(stage2.at[at("sp_0", nz, -d)], two + d, "sp_0")
        state = jnp.zeros((key, key), jnp.float32)
        for k in range(nz - 1):
            own = stage2[k]
            new = mul(own[:, key:], state) + own[:, 0:key].astype(jnp.float32)
            state = jnp.where(k < z, new, state)
        for k in range(ny):
            leaving[k] = low(state)
            if k < ny - 1:
                own = stage1[k]
                state = mul(own[:, key:], state) + own[:, 0:key].astype(jnp.float32)

    def share_states():
        for d in (2, 1, 3):
            to = at("sp_1", ny, d)
            links.start(leaving.at[to], incoming.at[y], three + d, "sp_1", to, lambda: leaving.at[0])
        keep_own.start()

    def delta_end():
        keep_own.wait()
        for d in range(1, ny):
            links.arrived(incoming.at[at("sp_1", ny, -d)], three + d, "sp_1")
        for s in range(nx):
            rows = mul(through[s], incoming[s]) + local_out[s]
            normed = (
                rows
                * lax.rsqrt(jnp.mean(rows * rows, axis=-1, keepdims=True) + NORM_EPS)
                * gain_ref[...]
            )
            delta_done[s] = low(normed)

    four = links.number(nx)
    keep_delta = pltpu.make_async_copy(delta_done.at[x], delta_in.at[x], local.at[4])

    def share_delta():
        for d in (2, 1, 3):
            to = at("fs", nx, d)
            links.start(delta_done.at[to], delta_in.at[x], four + d, "fs", to, lambda: delta_done.at[0])
        keep_delta.start()

    def key_row(row, count, diagonal):
        queries = rows_ref[...]
        beyond = None if diagonal else beyond_ref[...]
        weights = []
        for k in range(count - 1, -1, -1):
            scores = (
                jnp.dot(
                    queries,
                    kv_ref[row, 0:size, k * tile : (k + 1) * tile],
                    preferred_element_type=jnp.float32,
                )
                + offset
            )
            above = jnp.maximum(scores, 0.0)
            below = scores - above
            small = jnp.exp(below - above)
            log_term = jnp.where(small < 2.0**-12, small, jnp.log(1.0 + small))
            passed = above + log_term
            exponent = below - log_term
            if diagonal and k == count - 1:
                visible = col_at < row_at
                passed = jnp.where(visible, passed, 0.0)
                exponent = jnp.where(visible, exponent, -jnp.inf)
            after = jnp.dot(low(passed), later_ref[...], preferred_element_type=jnp.float32)
            exponent = exponent - after
            if beyond is not None:
                exponent = exponent - beyond
            total = after[:, :1] + passed[:, :1]
            beyond = total if beyond is None else beyond + total
            weights.append(low(jnp.exp(exponent)))
        partial = lax.dot_general(
            jnp.concatenate(weights[::-1], axis=1),
            kv_ref[row, size : 2 * size, 0 : count * tile],
            (((1,), (1,)), ((), ())),
            preferred_element_type=jnp.float32,
        )
        beyond_ref[...] = beyond
        if diagonal:
            acc_ref[...] = partial
        else:
            acc_ref[...] += partial

    five = links.number(2 * nx)
    sends = links.sent
    links.sent += nz
    home = z // 2
    slot = 2 * x + lax.rem(z, 2)

    def sb_copy(row):
        return pltpu.make_async_remote_copy(
            src_ref=done_ref.at[row],
            dst_ref=sb_in.at[slot],
            send_sem=send.at[sends + row],
            recv_sem=recv.at[five + slot],
            device_id={"fs": home, "sp_0": row},
            device_id_type=pl.DeviceIdType.MESH,
        )

    keep_sb = pltpu.make_async_copy(done_ref.at[z], sb_in.at[slot], local.at[5])

    def send_back(row):
        stays = (row == z) & (home == x)

        @pl.when(stays)
        def _():
            keep_sb.start()

        @pl.when(jnp.logical_not(stays))
        def _():
            sb_copy(row).start()

    def per_query(row, unused):
        rows_ref[...] = low((query_ref[row].astype(jnp.float32) * size ** (-0.5)).T)
        pl.when(row == 3)(over_group)
        pl.when(row == 6)(over_line)
        pl.when(row == 7)(delta_end)
        for k in range(groups):

            @pl.when(y == k)
            def _():
                key_row(row, k + 1, True)

        pl.when(row == 3)(share_group)
        pl.when(row == 6)(share_states)
        pl.when(row == 7)(share_delta)

        @pl.when(row > 0)
        def _():
            send_back(row - 1)

        def earlier(step, carried):
            key_row(row - 1 - step, groups, False)
            return carried

        lax.fori_loop(0, row, earlier, 0)
        done_ref[row] = low(acc_ref[...].T)
        return unused

    lax.fori_loop(0, nz, per_query, 0)
    for made in loads:
        made.wait()
    send_back(nz - 1)
    keep_delta.wait()
    for d in range(1, nx):
        links.arrived(delta_in.at[at("fs", nx, -d)], four + d, "fs")

    rows = tile // 2
    mine_rows = pl.ds(pl.multiple_of(t * rows, rows), rows)
    other_rows = pl.ds(pl.multiple_of((1 - t) * rows, rows), rows)
    delta_mixed = [delta_in[k] for k in range(nx)]
    columns = result_ref.shape[1]
    span = columns // 4
    for k in range(nx):
        for h in range(2):
            here = (z == 2 * x + h) & (x == k)

            @pl.when(here)
            def _():
                keep_sb.wait()

            @pl.when(jnp.logical_not(here))
            def _():
                links.arrived(sb_in.at[2 * k + h], five + 2 * k + h, "fs")

    sb_rows = sb_in[...].reshape(nz * size, tile).astype(jnp.float32).T
    rows_ref2 = low(jnp.concatenate([sb_rows] + [d.astype(jnp.float32) for d in delta_mixed], axis=1))
    taken[...] = rows_ref2
    six = links.number(4)

    def projected(part, cols):
        return low(
            jnp.dot(
                taken[part, 0 : nz * size], sb_out_w[:, cols], preferred_element_type=jnp.float32
            )
            + jnp.dot(
                taken[part, nz * size :], delta_out_w[:, cols], preferred_element_type=jnp.float32
            )
        )

    outs = [slice(c * span, (c + 1) * span) for c in range(4)]
    for c in range(4):
        given[0, :, outs[c]] = projected(other_rows, outs[c])
        if c:
            links.start(
                given.at[0, :, outs[c - 1]], given.at[1, :, outs[c - 1]], six + c - 1, "tp", 1 - t
            )
    own = projected(mine_rows, outs[0])
    links.start(given.at[0, :, outs[3]], given.at[1, :, outs[3]], six + 3, "tp", 1 - t)
    for c in range(4):
        links.arrived(given.at[1, :, outs[c]], six + c, "tp")
        total = own.astype(jnp.float32) + given[1, :, outs[c]].astype(jnp.float32)
        result_ref[:, outs[c]] = low(total)
        if c < 3:
            own = projected(mine_rows, outs[c + 1])
    for row in range(nz):

        @pl.when(jnp.logical_not((row == z) & (home == x)))
        def _():
            sb_copy(row).wait_send()

    links.drain()


def mix(offset, bias, scale, queries, keys_values, delta_proj, pre, shift, gain, sb_out, delta_out):
    nz, ny, nx = (lax.axis_size(a) for a in ("sp_0", "sp_1", "fs"))
    size, tile = queries.shape[1:]
    key = delta_proj.shape[2] // 3
    columns = sb_out.shape[1]
    half = tile // 2
    smem = pl.BlockSpec(memory_space=pltpu.SMEM)
    vmem = pl.BlockSpec(memory_space=pltpu.VMEM)
    anywhere = pl.BlockSpec(memory_space=pl.ANY)
    copies = 64
    bf16, f32 = jnp.bfloat16, jnp.float32
    return pl.pallas_call(
        mix_kernel,
        out_shape=jax.ShapeDtypeStruct((half, columns), bf16),
        in_specs=[smem] * 3 + [vmem] * 6 + [anywhere] * 2,
        out_specs=vmem,
        scratch_shapes=[
            pltpu.VMEM((tile, tile), bf16),
            pltpu.VMEM((tile, size), bf16),
            pltpu.VMEM((tile, size), f32),
            pltpu.VMEM((tile, 1), f32),
            pltpu.VMEM((nz, size, tile), bf16),
            pltpu.VMEM((2 * nx, size, tile), bf16),
            pltpu.VMEM((nx, tile, key), bf16),
            pltpu.VMEM((nx, tile, key), bf16),
            pltpu.VMEM((nx, tile, key), bf16),
            pltpu.VMEM((nx, tile, key), f32),
            pltpu.VMEM((nx, key, 2 * key), bf16),
            pltpu.VMEM((ny, key, 2 * key), bf16),
            pltpu.VMEM((nz, key, 2 * key), bf16),
            pltpu.VMEM((ny, key, key), bf16),
            pltpu.VMEM((nx, key, key), bf16),
            pltpu.VMEM(sb_out.shape, bf16),
            pltpu.VMEM(delta_out.shape, bf16),
            pltpu.VMEM((2, half, columns), bf16),
            pltpu.VMEM((tile, nz * size + nx * key), bf16),
            pltpu.SemaphoreType.DMA((copies,)),
            pltpu.SemaphoreType.DMA((copies,)),
            pltpu.SemaphoreType.DMA((6,)),
        ],
        compiler_params=pltpu.CompilerParams(collective_id=1, has_side_effects=True),
        name="mix",
        cost_estimate=pl.CostEstimate(
            flops=60_000_000_000, bytes_accessed=10_000_000, transcendentals=30_000_000
        ),
    )(offset, bias, scale, queries, keys_values, delta_proj, pre, shift, gain, sb_out, delta_out)


def on_device(
    hidden_in,
    sb_query_w,
    sb_key_w,
    sb_value_w,
    sb_offset,
    delta_query_w,
    delta_key_w,
    delta_value_w,
    decay_w,
    write_w,
    write_bias,
    decay_log_scale,
    decay_shift,
    head_gain,
    sb_out_w,
    delta_out_w,
):
    tokens, part = hidden_in.shape[1], hidden_in.shape[2]
    fs_count = lax.axis_size("fs")
    mine = lax.axis_index("fs")
    gates_w = jnp.concatenate(
        [lax.dynamic_slice_in_dim(w, mine, 1, 1) for w in (decay_w, write_w)], axis=1
    )
    lanes = sb_query_w.shape[1] // fs_count
    gates_w = jnp.pad(gates_w, ((0, 0), (0, lanes - 2))).reshape(fs_count, -1, lanes)
    unit_queries, keys_values, delta_proj, pre, shift = project_and_share(
        hidden_in.reshape(tokens, part),
        gates_w,
        decay_shift.reshape(fs_count, 1, tokens),
        (sb_query_w, sb_key_w, sb_value_w),
        (delta_query_w, delta_key_w, delta_value_w),
    )
    result = mix(
        sb_offset,
        write_bias,
        decay_log_scale,
        unit_queries,
        keys_values,
        delta_proj,
        pre,
        shift,
        head_gain.reshape(1, -1),
        sb_out_w,
        delta_out_w,
    )
    return result.reshape(1, *result.shape)


def solution(mesh):
    finer = Mesh(
        mesh.devices.reshape(8, 4, mesh.shape["fs"], mesh.shape["tp"]), ("sp_0", "sp_1", "fs", "tp")
    )
    return jax.shard_map(
        on_device,
        mesh=finer,
        in_specs=(
            P("fs", SP, "tp"),
            P("fs", "tp"),
            P("fs", "tp"),
            P("fs", "tp"),
            P("tp"),
            P("fs", "tp"),
            P("fs", "tp"),
            P("fs", "tp"),
            P(None, "tp"),
            P(None, "tp"),
            P("tp"),
            P("tp"),
            P("fs", "tp", SP),
            P(),
            P("tp", None),
            P("tp", None),
        ),
        out_specs=P("fs", SP_TP, None),
        check_vma=False,
    )
```

```python
import jax
import jax.numpy as jnp
from jax import lax
from jax.experimental import pallas as pl
from jax.experimental.pallas import tpu as pltpu
from jax.sharding import Mesh
from jax.sharding import PartitionSpec as P

SB_DIM = 64
GDN_DIM = 128
BLOCK = 64
SP = ("sp_0", "sp_1")
SP_TP = ("sp_0", "sp_1", "tp")
NORM_EPS = 1e-06


def unit_rows(vectors):
    return vectors * lax.rsqrt(jnp.sum(vectors * vectors, axis=-1, keepdims=True) + NORM_EPS)


class Links:
    def __init__(self, send, recv, me):
        self.me = me
        self.send, self.recv, self.count, self.sent, self.open = send, recv, 0, 0, []

    def number(self, n=1):
        self.count += n
        return self.count - n

    def copy(self, src, dst, k, axis, to):
        return pltpu.make_async_remote_copy(
            src_ref=src,
            dst_ref=dst,
            send_sem=self.send.at[self.sent],
            recv_sem=self.recv.at[k],
            device_id={axis: to},
            device_id_type=pl.DeviceIdType.MESH,
        )

    def start(self, src, dst, k, axis, to, like=None):
        made = self.copy(src, dst, k, axis, to)
        made.start()
        self.open.append((made, self.sent, like, axis))
        self.sent += 1

    def arrived(self, dst, k, axis):
        self.copy(dst, dst, k, axis, self.me[axis]).wait_recv()

    def drain(self):
        for made, sent, like, axis in self.open:
            if like is not None:
                self.sent = sent
                made = self.copy(like(), like(), 0, axis, self.me[axis])
            made.wait_send()
        self.open = []


def layer_kernel(
    offset_ref, bias_ref, scale_ref, hidden_ref, decay_ref, write_ref, shift_in, gain_ref,
    q0, k0, v0, q1, k1, v1, sb_out_ref, delta_out_ref,
    result_ref,
    acts, sb_w, delta_w, units, query_ref, kv_ref, delta_ref, pre_ref, shift_out, shift_ref,
    later_ref, rows_ref, acc_ref, beyond_ref, done_ref, sb_in, delta_in, delta_done,
    through, local_out, transfer, stage1, stage2, leaving, incoming,
    sb_out_w, delta_out_w, given, taken, send, recv, local,
):
    z, y, x, t = (lax.axis_index(a) for a in ("sp_0", "sp_1", "fs", "tp"))
    nz, ny, nx = (lax.axis_size(a) for a in ("sp_0", "sp_1", "fs"))
    me = {"sp_0": z, "sp_1": y, "fs": x, "tp": t}
    links = Links(send, recv, me)
    tile, size = query_ref.shape[2], query_ref.shape[1]
    tokens, half = tile, tile // 2
    groups = kv_ref.shape[2] // tile
    key = delta_ref.shape[2] // 3
    lanes = q0.shape[1] // nx
    width = 3 * lanes
    z_rows, y_rows = q0.shape[0] // nz, q0.shape[0] // ny

    def at(axis, count, by):
        return lax.rem(me[axis] + by + count, count)

    def low(a):
        return a.astype(jnp.bfloat16)

    barrier = pltpu.get_barrier_semaphore()
    peers = [
        {"sp_0": at("sp_0", nz, dz), "fs": at("fs", nx, dx)}
        for dz in range(nz)
        for dx in range(nx)
        if dz or dx
    ]
    peers += [{"sp_1": at("sp_1", ny, d)} for d in range(1, ny)] + [{"tp": 1 - t}]
    for peer in peers:
        pl.semaphore_signal(barrier, inc=1, device_id=peer, device_id_type=pl.DeviceIdType.MESH)
    pl.semaphore_wait(barrier, len(peers))

    sets = (
        ((q0, k0), sb_w, 0, z * z_rows, z_rows),
        ((v0,), sb_w, 2, y * y_rows, y_rows),
        ((q1, k1, v1), delta_w, 0, y * y_rows, y_rows),
    )
    first = {}
    own = []

    def pass_on(s, d):
        mats, held, place, row, count = sets[s]
        to = at("fs", nx, d)
        first[s, d] = links.number()
        for m, w in enumerate(mats):
            src = w.at[pl.ds(row, count), pl.ds(pl.multiple_of(to * lanes, lanes), lanes)]
            cols = slice((place + m) * lanes, (place + m + 1) * lanes)
            dst = held.at[x, pl.ds(row, count), cols]
            if d:
                links.start(src, dst, first[s, d], "fs", to)
            else:
                own.append(pltpu.make_async_copy(src, dst, local.at[6 + len(own)]))
                own[-1].start()

    for d in (2, 1, 3, 0):
        pass_on(0, d)
        pass_on(1, d)
    for d in (2, 1, 3, 0):
        pass_on(2, d)
    right, left, other = at("fs", nx, 1), at("fs", nx, -1), 1 - t
    act = links.number(8)
    links.start(hidden_ref, acts.at[x, t], act, "fs", right)
    links.start(hidden_ref, acts.at[x, t], act + 1, "fs", left)
    links.start(hidden_ref, acts.at[x, t], act + 4, "tp", other)
    keep = pltpu.make_async_copy(hidden_ref, acts.at[x, t], local.at[12])
    keep.start()
    loads = [
        pltpu.make_async_copy(sb_out_ref, sb_out_w, local.at[0]),
        pltpu.make_async_copy(delta_out_ref, delta_out_w, local.at[1]),
    ]
    for s in range(nx):
        shift_out[s] = shift_in[s : s + 1]
    gates = jnp.concatenate(
        [
            decay_ref[...].astype(jnp.float32),
            write_ref[...].astype(jnp.float32),
            jnp.zeros((lanes - 2 * nx, decay_ref.shape[1]), jnp.float32),
        ],
        axis=0,
    )
    delta_w[:, :, width : width + lanes] = low(gates.T).reshape(nx, -1, lanes)
    row_at = lax.broadcasted_iota(jnp.int32, (tile, tile), 0)
    col_at = lax.broadcasted_iota(jnp.int32, (tile, tile), 1)
    later_ref[...] = jnp.where(row_at > col_at, 1.0, 0.0).astype(jnp.bfloat16)
    offset = offset_ref[2 * x + lax.rem(z, 2)]

    z_right, z_left = at("sp_0", nz, 1), at("sp_0", nz, -1)
    y_right, y_left = at("sp_1", ny, 1), at("sp_1", ny, -1)
    steps = nz // 2
    zr, zl = links.number(steps), links.number(steps)
    vr, vl, dr, dl = (links.number(2) for _ in range(4))

    def sb_piece(by, lo=0, count=nx):
        rows = pl.ds(at("sp_0", nz, by) * z_rows, z_rows)
        return sb_w.at[lo : lo + count, rows, 0 : 2 * lanes]

    def v_piece(by, lo=0, count=nx):
        rows = pl.ds(at("sp_1", ny, by) * y_rows, y_rows)
        return sb_w.at[lo : lo + count, rows, 2 * lanes : width]

    def delta_piece(by, lo=0, count=nx):
        rows = pl.ds(at("sp_1", ny, by) * y_rows, y_rows)
        return delta_w.at[lo : lo + count, rows, 0:width]

    def come(s, rows):
        mats, held, place, row, count = sets[s]
        for d in (1, 3, 2):
            links.arrived(
                held.at[
                    at("fs", nx, -d), pl.ds(row, count),
                    place * lanes : (place + len(mats)) * lanes,
                ],
                first[s, d], "fs",
            )

    def y_start(piece, r, l):
        links.start(piece(0), piece(0), r, "sp_1", y_right)
        links.start(piece(0), piece(0), l, "sp_1", y_left)

    def y_step(piece, r, l):
        links.arrived(piece(-1), r, "sp_1")
        links.start(piece(-1, 0, 2), piece(-1, 0, 2), r + 1, "sp_1", y_right)
        links.arrived(piece(1), l, "sp_1")
        links.start(piece(1, 2, 2), piece(1, 2, 2), l + 1, "sp_1", y_left)

    def y_end(piece, r, l):
        links.arrived(piece(2, 0, 2), r + 1, "sp_1")
        links.arrived(piece(2, 2, 2), l + 1, "sp_1")

    def z_step(s):
        if s < steps:
            lo, count = (0, nx) if s < steps - 1 else (0, nx // 2)
            links.arrived(sb_piece(-s), zr + s - 1, "sp_0")
            links.start(sb_piece(-s, lo, count), sb_piece(-s, lo, count), zr + s, "sp_0", z_right)
            lo, count = (0, nx) if s < steps - 1 else (nx // 2, nx // 2)
            links.arrived(sb_piece(s), zl + s - 1, "sp_0")
            links.start(sb_piece(s, lo, count), sb_piece(s, lo, count), zl + s, "sp_0", z_left)
        else:
            links.arrived(sb_piece(steps, 0, nx // 2), zr + s - 1, "sp_0")
            links.arrived(sb_piece(steps, nx // 2, nx // 2), zl + s - 1, "sp_0")

    for made in own:
        made.wait()
    come(0, z_rows)
    links.start(sb_piece(0), sb_piece(0), zr, "sp_0", z_right)
    links.start(sb_piece(0), sb_piece(0), zl, "sp_0", z_left)
    come(1, y_rows)
    y_start(v_piece, vr, vl)
    shifts = links.number(nx)
    for d in range(1, nx):
        to = at("fs", nx, d)
        links.start(shift_out.at[to], shift_ref.at[x], shifts + d, "fs", to)
    keep_shift = pltpu.make_async_copy(shift_out.at[x], shift_ref.at[x], local.at[13])
    keep_shift.start()
    come(2, y_rows)
    y_start(delta_piece, dr, dl)
    z_step(1)
    y_step(v_piece, vr, vl)
    z_step(2)
    before, after, far = at("fs", nx, -1), at("fs", nx, 1), at("fs", nx, 2)
    links.arrived(acts.at[before, t], act, "fs")
    links.start(acts.at[before, t, 0:half], acts.at[before, t, 0:half], act + 2, "fs", right)
    links.start(acts.at[before, t], acts.at[before, t], act + 5, "tp", other)
    links.arrived(acts.at[after, t], act + 1, "fs")
    links.start(
        acts.at[after, t, half:tokens], acts.at[after, t, half:tokens], act + 3, "fs", left
    )
    links.start(acts.at[after, t], acts.at[after, t], act + 6, "tp", other)
    for made in loads:
        made.start()
    z_step(3)
    y_step(delta_piece, dr, dl)
    y_end(v_piece, vr, vl)
    z_step(4)
    keep.wait()

    def product(c, held):
        return sum(
            jnp.dot(
                acts[c, p],
                held[2 * p : 2 * p + 2].reshape(acts.shape[3], -1),
                preferred_element_type=jnp.float32,
            )
            for p in range(2)
        )

    def sb_sequence(c):
        out = product(c, sb_w)
        for m in range(3):
            block = low(out[:, m * lanes : (m + 1) * lanes].T)
            units[2 * c, m * size : (m + 1) * size, :] = block[0:size]
            units[2 * c + 1, m * size : (m + 1) * size, :] = block[size:lanes]

    def delta_sequence(c):
        out = product(c, delta_w)
        delta_ref[c] = low(out[:, 0:width])
        pre_ref[c] = out[:, width : width + lanes].T[0:8]

    def near(i, carried):
        c = lax.rem(x + i + nx - 1, nx)
        sb_sequence(c)
        return carried

    for k, c in enumerate((x, before, after)):
        links.arrived(acts.at[c, other], act + 4 + k, "tp")
    lax.fori_loop(0, 3, near, 0)
    links.arrived(acts.at[far, t, 0:half], act + 2, "fs")
    links.arrived(acts.at[far, t, half:tokens], act + 3, "fs")
    links.start(acts.at[far, t], acts.at[far, t], act + 7, "tp", other)
    y_end(delta_piece, dr, dl)
    links.arrived(acts.at[far, other], act + 7, "tp")
    lax.fori_loop(3, 4, near, 0)
    delta_sequence(x)

    here = pl.ds(pl.multiple_of(y * tokens, tokens), tokens)
    zq, zk = links.number(nz), links.number(nz)
    order = (4, 3, 5, 2, 6, 1, 7)
    mine_units = (
        pltpu.make_async_copy(units.at[z, 0:size], query_ref.at[z], local.at[14]),
        pltpu.make_async_copy(units.at[z, size : 3 * size], kv_ref.at[z, :, here], local.at[15]),
    )
    for d in order:
        to = at("sp_0", nz, d)
        links.start(units.at[to, size : 3 * size], kv_ref.at[z, :, here], zk + d, "sp_0", to)
    for made in mine_units:
        made.start()
    for d in order:
        to = at("sp_0", nz, d)
        links.start(units.at[to, 0:size], query_ref.at[z], zq + d, "sp_0", to)

    kv_r, kv_l = links.number(nz), links.number(nz)
    kv_rr, kv_ll = links.number(nz), links.number(nz)

    def kv_piece(row, by, lo=0, count=2 * size):
        cols = pl.ds(pl.multiple_of(at("sp_1", ny, by) * tokens, tokens), tokens)
        return kv_ref.at[row, lo : lo + count, cols]

    def give(d):
        row = at("sp_0", nz, -d)
        if d:
            links.arrived(kv_ref.at[row, :, here], zk + d, "sp_0")
        links.start(kv_piece(row, 0), kv_piece(row, 0), kv_r + d, "sp_1", y_right)
        links.start(kv_piece(row, 0), kv_piece(row, 0), kv_l + d, "sp_1", y_left)

    def forward(d):
        row = at("sp_0", nz, -d)
        links.arrived(kv_piece(row, -1), kv_r + d, "sp_1")
        links.start(
            kv_piece(row, -1, 0, size), kv_piece(row, -1, 0, size), kv_rr + d, "sp_1", y_right
        )
        links.arrived(kv_piece(row, 1), kv_l + d, "sp_1")
        links.start(
            kv_piece(row, 1, size, size), kv_piece(row, 1, size, size), kv_ll + d, "sp_1", y_left
        )

    def delta_next(i, carried):
        delta_sequence(lax.rem(x + i, nx))
        return carried

    for made in mine_units:
        made.wait()
    give(0)
    lax.fori_loop(1, nx, delta_next, 0)
    keep_shift.wait()
    for d in range(1, nx):
        links.arrived(shift_ref.at[at("fs", nx, -d)], shifts + d, "fs")

    def mul(a, b, contract=((1,), (0,))):
        return lax.dot_general(
            low(a), low(b), (contract, ((), ())), preferred_element_type=jnp.float32
        )

    same = row_at // BLOCK == col_at // BLOCK
    inclusive = same & (col_at <= row_at)
    strictly = same & (col_at < row_at)
    decay_pre = jnp.concatenate([pre_ref[s, pl.ds(x, 1)] for s in range(nx)], axis=0)
    write_pre = jnp.concatenate([pre_ref[s, pl.ds(nx + x, 1)] for s in range(nx)], axis=0)
    shift = jnp.concatenate([shift_ref[s] for s in range(nx)], axis=0)
    softplus = jnp.maximum(decay_pre, 0.0) + jnp.log1p(jnp.exp(-jnp.abs(decay_pre)))
    rate = jnp.exp(jnp.full(decay_pre.shape, scale_ref[x], jnp.float32))
    log_decay = shift - rate * softplus
    strength = jax.nn.sigmoid(write_pre + bias_ref[x])
    up_to = jnp.where(same & (row_at <= col_at), 1.0, 0.0)
    both = jnp.concatenate([log_decay, strength], axis=0)
    summed = jnp.dot(
        both, up_to, preferred_element_type=jnp.float32, precision=lax.Precision.HIGHEST
    )
    sums_col = summed.T
    both_col = both.T
    blocks = tile // BLOCK

    def local_part(s):
        cum_row = summed[s : s + 1]
        cum = sums_col[:, s : s + 1]
        beta = both_col[:, nx + s : nx + s + 1]
        act = jax.nn.silu(delta_ref[s].astype(jnp.float32))
        q, k, v = act[:, 0:key], act[:, key : 2 * key], act[:, 2 * key : 3 * key]
        q = unit_rows(q) * key ** (-0.5)
        k = unit_rows(k)
        spread = cum - cum_row
        decay = jnp.where(inclusive, jnp.exp(jnp.where(inclusive, spread, 0.0)), 0.0)
        k_beta = k * beta
        lower = jnp.where(strictly, mul(k_beta, k, ((1,), (1,))) * decay, 0.0)
        inside = mul(q, k, ((1,), (1,))) * decay
        powered = lower
        inverse = jnp.where(row_at == col_at, 1.0, 0.0) - lower
        for _ in range(max(1, (BLOCK - 1).bit_length()) - 1):
            powered = mul(powered, powered)
            inverse = inverse + mul(inverse, powered)
        growth = jnp.exp(cum)
        updates = mul(inverse, jnp.concatenate([v * beta, k_beta * growth], axis=1))
        within = mul(inside, updates)
        reach = q * growth - within[:, key:]
        last = [cum[(b + 1) * BLOCK - 1 : (b + 1) * BLOCK] for b in range(blocks)]
        carried = None
        eye = jnp.where(
            lax.broadcasted_iota(jnp.int32, (key, key), 0)
            == lax.broadcasted_iota(jnp.int32, (key, key), 1),
            1.0,
            0.0,
        )
        zero = jnp.zeros((key, key), jnp.float32)
        for b in range(blocks):
            rows = slice(b * BLOCK, (b + 1) * BLOCK)
            damped = k[rows] * jnp.exp(last[b] - cum[rows])
            step = mul(damped, updates[rows], ((0,), (0,)))
            keep = jnp.exp(last[b])
            start = jnp.concatenate([zero, eye], axis=1) if carried is None else carried
            out = mul(reach[rows], start)
            local_out[s, rows] = within[rows, 0:key] + out[:, 0:key]
            through[s, rows] = low(out[:, key:])
            carried = (
                start * keep
                - mul(step[:, key:], start)
                + jnp.concatenate([step[:, 0:key], zero], axis=1)
            )
        transfer[s] = low(carried)

    give(4)
    local_part(0)
    give(3)
    give(5)
    forward(0)
    local_part(1)
    give(2)
    give(6)
    forward(4)
    forward(3)
    local_part(2)
    give(1)
    give(7)
    forward(5)
    forward(2)
    local_part(3)
    forward(6)
    forward(1)
    forward(7)

    one = links.number(ny)
    for d in (2, 1, 3):
        to = at("sp_1", ny, d)
        links.start(transfer.at[to], stage1.at[y], one + d, "sp_1", to)
    mine = pltpu.make_async_copy(transfer.at[y], stage1.at[y], local.at[2])
    mine.start()
    for d in (0,) + order:
        row = at("sp_0", nz, -d)
        if d:
            links.arrived(query_ref.at[row], zq + d, "sp_0")
        links.arrived(kv_piece(row, 2, 0, size), kv_rr + d, "sp_1")
        links.arrived(kv_piece(row, 2, size, size), kv_ll + d, "sp_1")
    two, three = links.number(nz), links.number(ny)
    keep_own = pltpu.make_async_copy(leaving.at[y], incoming.at[y], local.at[3])

    def over_group():
        mine.wait()
        for d in range(1, ny):
            links.arrived(stage1.at[at("sp_1", ny, -d)], one + d, "sp_1")
        joined = stage1[0].astype(jnp.float32)
        for k in range(1, ny):
            own = stage1[k]
            new = mul(own[:, key:], joined)
            joined = jnp.concatenate(
                [new[:, 0:key] + own[:, 0:key].astype(jnp.float32), new[:, key:]], axis=1
            )
        stage2[z] = low(joined)

    def share_group():
        for d in (4, 3, 5, 2, 6, 1, 7):
            links.start(stage2.at[z], stage2.at[z], two + d, "sp_0", at("sp_0", nz, d), lambda: stage2.at[0])

    def over_line():
        for d in range(1, nz):
            links.arrived(stage2.at[at("sp_0", nz, -d)], two + d, "sp_0")
        state = jnp.zeros((key, key), jnp.float32)
        for k in range(nz - 1):
            own = stage2[k]
            new = mul(own[:, key:], state) + own[:, 0:key].astype(jnp.float32)
            state = jnp.where(k < z, new, state)
        for k in range(ny):
            leaving[k] = low(state)
            if k < ny - 1:
                own = stage1[k]
                state = mul(own[:, key:], state) + own[:, 0:key].astype(jnp.float32)

    def share_states():
        for d in (2, 1, 3):
            to = at("sp_1", ny, d)
            links.start(leaving.at[to], incoming.at[y], three + d, "sp_1", to, lambda: leaving.at[0])
        keep_own.start()

    def delta_end():
        keep_own.wait()
        for d in range(1, ny):
            links.arrived(incoming.at[at("sp_1", ny, -d)], three + d, "sp_1")
        for s in range(nx):
            rows = mul(through[s], incoming[s]) + local_out[s]
            normed = (
                rows
                * lax.rsqrt(jnp.mean(rows * rows, axis=-1, keepdims=True) + NORM_EPS)
                * gain_ref[...]
            )
            delta_done[s] = low(normed)

    four = links.number(nx)
    keep_delta = pltpu.make_async_copy(delta_done.at[x], delta_in.at[x], local.at[4])

    def share_delta():
        for d in (2, 1, 3):
            to = at("fs", nx, d)
            links.start(delta_done.at[to], delta_in.at[x], four + d, "fs", to, lambda: delta_done.at[0])
        keep_delta.start()

    def key_row(row, count, diagonal):
        queries = rows_ref[...]
        beyond = None if diagonal else beyond_ref[...]
        weights = []
        for k in range(count - 1, -1, -1):
            scores = (
                jnp.dot(
                    queries,
                    kv_ref[row, 0:size, k * tile : (k + 1) * tile],
                    preferred_element_type=jnp.float32,
                )
                + offset
            )
            above = jnp.maximum(scores, 0.0)
            below = scores - above
            small = jnp.exp(below - above)
            log_term = jnp.where(small < 2.0**-12, small, jnp.log(1.0 + small))
            passed = above + log_term
            exponent = below - log_term
            if diagonal and k == count - 1:
                visible = col_at < row_at
                passed = jnp.where(visible, passed, 0.0)
                exponent = jnp.where(visible, exponent, -jnp.inf)
            after = jnp.dot(low(passed), later_ref[...], preferred_element_type=jnp.float32)
            exponent = exponent - after
            if beyond is not None:
                exponent = exponent - beyond
            total = after[:, :1] + passed[:, :1]
            beyond = total if beyond is None else beyond + total
            weights.append(low(jnp.exp(exponent)))
        partial = lax.dot_general(
            jnp.concatenate(weights[::-1], axis=1),
            kv_ref[row, size : 2 * size, 0 : count * tile],
            (((1,), (1,)), ((), ())),
            preferred_element_type=jnp.float32,
        )
        beyond_ref[...] = beyond
        if diagonal:
            acc_ref[...] = partial
        else:
            acc_ref[...] += partial

    five = links.number(2 * nx)
    sends = links.sent
    links.sent += nz
    home = z // 2
    slot = 2 * x + lax.rem(z, 2)

    def sb_copy(row):
        return pltpu.make_async_remote_copy(
            src_ref=done_ref.at[row],
            dst_ref=sb_in.at[slot],
            send_sem=send.at[sends + row],
            recv_sem=recv.at[five + slot],
            device_id={"fs": home, "sp_0": row},
            device_id_type=pl.DeviceIdType.MESH,
        )

    keep_sb = pltpu.make_async_copy(done_ref.at[z], sb_in.at[slot], local.at[5])

    def send_back(row):
        stays = (row == z) & (home == x)

        @pl.when(stays)
        def _():
            keep_sb.start()

        @pl.when(jnp.logical_not(stays))
        def _():
            sb_copy(row).start()

    def per_query(row, unused):
        rows_ref[...] = low((query_ref[row].astype(jnp.float32) * size ** (-0.5)).T)
        pl.when(row == 3)(over_group)
        pl.when(row == 6)(over_line)
        pl.when(row == 7)(delta_end)
        for k in range(groups):

            @pl.when(y == k)
            def _():
                key_row(row, k + 1, True)

        pl.when(row == 3)(share_group)
        pl.when(row == 6)(share_states)
        pl.when(row == 7)(share_delta)

        @pl.when(row > 0)
        def _():
            send_back(row - 1)

        def earlier(step, carried):
            key_row(row - 1 - step, groups, False)
            return carried

        lax.fori_loop(0, row, earlier, 0)
        done_ref[row] = low(acc_ref[...].T)
        return unused

    lax.fori_loop(0, nz, per_query, 0)
    for made in loads:
        made.wait()
    send_back(nz - 1)
    keep_delta.wait()
    for d in range(1, nx):
        links.arrived(delta_in.at[at("fs", nx, -d)], four + d, "fs")

    rows = tile // 2
    mine_rows = pl.ds(pl.multiple_of(t * rows, rows), rows)
    other_rows = pl.ds(pl.multiple_of((1 - t) * rows, rows), rows)
    delta_mixed = [delta_in[k] for k in range(nx)]
    columns = result_ref.shape[1]
    span = columns // 4
    for k in range(nx):
        for h in range(2):
            here = (z == 2 * x + h) & (x == k)

            @pl.when(here)
            def _():
                keep_sb.wait()

            @pl.when(jnp.logical_not(here))
            def _():
                links.arrived(sb_in.at[2 * k + h], five + 2 * k + h, "fs")

    sb_rows = sb_in[...].reshape(nz * size, tile).astype(jnp.float32).T
    rows_ref2 = low(jnp.concatenate([sb_rows] + [d.astype(jnp.float32) for d in delta_mixed], axis=1))
    taken[...] = rows_ref2
    six = links.number(4)

    def projected(part, cols):
        return low(
            jnp.dot(
                taken[part, 0 : nz * size], sb_out_w[:, cols], preferred_element_type=jnp.float32
            )
            + jnp.dot(
                taken[part, nz * size :], delta_out_w[:, cols], preferred_element_type=jnp.float32
            )
        )

    outs = [slice(c * span, (c + 1) * span) for c in range(4)]
    for c in range(4):
        given[0, :, outs[c]] = projected(other_rows, outs[c])
        if c:
            links.start(
                given.at[0, :, outs[c - 1]], given.at[1, :, outs[c - 1]], six + c - 1, "tp", 1 - t
            )
    own = projected(mine_rows, outs[0])
    links.start(given.at[0, :, outs[3]], given.at[1, :, outs[3]], six + 3, "tp", 1 - t)
    for c in range(4):
        links.arrived(given.at[1, :, outs[c]], six + c, "tp")
        total = own.astype(jnp.float32) + given[1, :, outs[c]].astype(jnp.float32)
        result_ref[:, outs[c]] = low(total)
        if c < 3:
            own = projected(mine_rows, outs[c + 1])
    for row in range(nz):

        @pl.when(jnp.logical_not((row == z) & (home == x)))
        def _():
            sb_copy(row).wait_send()

    links.drain()


def layer(offset, bias, scale, hidden, decay, write, shift, gain, sb_w, delta_w, sb_out, delta_out):
    nz, ny, nx = (lax.axis_size(a) for a in ("sp_0", "sp_1", "fs"))
    tile, part = hidden.shape
    rows, lanes = sb_w[0].shape[0], sb_w[0].shape[1] // nx
    size, key = lanes // 2, lanes
    columns = sb_out.shape[1]
    half = tile // 2
    smem = pl.BlockSpec(memory_space=pltpu.SMEM)
    vmem = pl.BlockSpec(memory_space=pltpu.VMEM)
    anywhere = pl.BlockSpec(memory_space=pl.ANY)
    copies = 160
    bf16, f32 = jnp.bfloat16, jnp.float32
    return pl.pallas_call(
        layer_kernel,
        out_shape=jax.ShapeDtypeStruct((half, columns), bf16),
        in_specs=[smem] * 3 + [vmem] * 5 + [anywhere] * 8,
        out_specs=vmem,
        scratch_shapes=[
            pltpu.VMEM((nx, 2, tile, part), bf16),
            pltpu.VMEM((nx, rows, 3 * lanes), bf16),
            pltpu.VMEM((nx, rows, 4 * lanes), bf16),
            pltpu.VMEM((nz, 3 * size, tile), bf16),
            pltpu.VMEM((nz, size, tile), bf16),
            pltpu.VMEM((nz, 2 * size, ny * tile), bf16),
            pltpu.VMEM((nx, tile, 3 * key), bf16),
            pltpu.VMEM((nx, 8, tile), f32),
            pltpu.VMEM((nx, 1, tile), f32),
            pltpu.VMEM((nx, 1, tile), f32),
            pltpu.VMEM((tile, tile), bf16),
            pltpu.VMEM((tile, size), bf16),
            pltpu.VMEM((tile, size), f32),
            pltpu.VMEM((tile, 1), f32),
            pltpu.VMEM((nz, size, tile), bf16),
            pltpu.VMEM((2 * nx, size, tile), bf16),
            pltpu.VMEM((nx, tile, key), bf16),
            pltpu.VMEM((nx, tile, key), bf16),
            pltpu.VMEM((nx, tile, key), bf16),
            pltpu.VMEM((nx, tile, key), f32),
            pltpu.VMEM((nx, key, 2 * key), bf16),
            pltpu.VMEM((ny, key, 2 * key), bf16),
            pltpu.VMEM((nz, key, 2 * key), bf16),
            pltpu.VMEM((ny, key, key), bf16),
            pltpu.VMEM((nx, key, key), bf16),
            pltpu.VMEM(sb_out.shape, bf16),
            pltpu.VMEM(delta_out.shape, bf16),
            pltpu.VMEM((2, half, columns), bf16),
            pltpu.VMEM((tile, nz * size + nx * key), bf16),
            pltpu.SemaphoreType.DMA((copies,)),
            pltpu.SemaphoreType.DMA((copies,)),
            pltpu.SemaphoreType.DMA((16,)),
        ],
        compiler_params=pltpu.CompilerParams(collective_id=0, has_side_effects=True),
        name="layer",
    )(offset, bias, scale, hidden, decay, write, shift, gain, *sb_w, *delta_w, sb_out, delta_out)


def on_device(
    hidden_in,
    sb_query_w,
    sb_key_w,
    sb_value_w,
    sb_offset,
    delta_query_w,
    delta_key_w,
    delta_value_w,
    decay_w,
    write_w,
    write_bias,
    decay_log_scale,
    decay_shift,
    head_gain,
    sb_out_w,
    delta_out_w,
):
    tokens, part = hidden_in.shape[1], hidden_in.shape[2]
    result = layer(
        sb_offset,
        write_bias,
        decay_log_scale,
        hidden_in.reshape(tokens, part),
        decay_w.T,
        write_w.T,
        decay_shift.reshape(-1, tokens),
        head_gain.reshape(1, -1),
        (sb_query_w, sb_key_w, sb_value_w),
        (delta_query_w, delta_key_w, delta_value_w),
        sb_out_w,
        delta_out_w,
    )
    return result.reshape(1, *result.shape)


def solution(mesh):
    finer = Mesh(
        mesh.devices.reshape(8, 4, mesh.shape["fs"], mesh.shape["tp"]), ("sp_0", "sp_1", "fs", "tp")
    )
    return jax.shard_map(
        on_device,
        mesh=finer,
        in_specs=(
            P("fs", SP, "tp"),
            P("fs", "tp"),
            P("fs", "tp"),
            P("fs", "tp"),
            P("tp"),
            P("fs", "tp"),
            P("fs", "tp"),
            P("fs", "tp"),
            P(None, "tp"),
            P(None, "tp"),
            P("tp"),
            P("tp"),
            P("fs", "tp", SP),
            P(),
            P("tp", None),
            P("tp", None),
        ),
        out_specs=P("fs", SP_TP, None),
        check_vma=False,
    )
```

```python
import jax
import jax.numpy as jnp
from jax import lax
from jax.experimental import pallas as pl
from jax.experimental.pallas import tpu as pltpu
from jax.sharding import Mesh
from jax.sharding import PartitionSpec as P

SB_DIM = 64
GDN_DIM = 128
BLOCK = 64
SP = ("sp_0", "sp_1")
SP_TP = ("sp_0", "sp_1", "tp")
NORM_EPS = 1e-06


def unit_rows(vectors):
    return vectors * lax.rsqrt(jnp.sum(vectors * vectors, axis=-1, keepdims=True) + NORM_EPS)


class Links:
    def __init__(self, send, recv, me):
        self.me = me
        self.send, self.recv, self.count, self.sent, self.open = send, recv, 0, 0, []

    def number(self, n=1):
        self.count += n
        return self.count - n

    def copy(self, src, dst, k, axis, to):
        return pltpu.make_async_remote_copy(
            src_ref=src,
            dst_ref=dst,
            send_sem=self.send.at[self.sent],
            recv_sem=self.recv.at[k],
            device_id={axis: to},
            device_id_type=pl.DeviceIdType.MESH,
        )

    def start(self, src, dst, k, axis, to, like=None):
        made = self.copy(src, dst, k, axis, to)
        made.start()
        self.open.append((made, self.sent, like, axis))
        self.sent += 1

    def arrived(self, dst, k, axis):
        self.copy(dst, dst, k, axis, self.me[axis]).wait_recv()

    def drain(self):
        for made, sent, like, axis in self.open:
            if like is not None:
                self.sent = sent
                made = self.copy(like(), like(), 0, axis, self.me[axis])
            made.wait_send()
        self.open = []


def layer_kernel(
    offset_ref, bias_ref, scale_ref, hidden_ref, decay_ref, write_ref, shift_in, gain_ref,
    q0, k0, v0, q1, k1, v1, sb_out_ref, delta_out_ref,
    result_ref,
    acts, sb_w, delta_w, units, query_ref, kv_ref, delta_ref, pre_ref, shift_out, shift_ref,
    later_ref, rows_ref, acc_ref, beyond_ref, done_ref, sb_in, delta_in, delta_done,
    through, local_out, transfer, stage1, stage2, leaving, incoming,
    sb_out_w, delta_out_w, given, taken, send, recv, local,
):
    z, y, x, t = (lax.axis_index(a) for a in ("sp_0", "sp_1", "fs", "tp"))
    nz, ny, nx = (lax.axis_size(a) for a in ("sp_0", "sp_1", "fs"))
    me = {"sp_0": z, "sp_1": y, "fs": x, "tp": t}
    links = Links(send, recv, me)
    tile, size = query_ref.shape[2], query_ref.shape[1]
    tokens, half = tile, tile // 2
    groups = kv_ref.shape[2] // tile
    key = delta_ref.shape[2] // 3
    lanes = q0.shape[1] // nx
    width = 3 * lanes
    extra = kv_ref.shape[1] - 2 * size
    z_rows, y_rows = q0.shape[0] // nz, q0.shape[0] // ny

    def at(axis, count, by):
        return lax.rem(me[axis] + by + count, count)

    def low(a):
        return a.astype(jnp.bfloat16)

    barrier = pltpu.get_barrier_semaphore()
    peers = [
        {"sp_0": at("sp_0", nz, dz), "fs": at("fs", nx, dx)}
        for dz in range(nz)
        for dx in range(nx)
        if dz or dx
    ]
    peers += [{"sp_1": at("sp_1", ny, d)} for d in range(1, ny)] + [{"tp": 1 - t}]
    for peer in peers:
        pl.semaphore_signal(barrier, inc=1, device_id=peer, device_id_type=pl.DeviceIdType.MESH)
    pl.semaphore_wait(barrier, len(peers))

    sets = (
        ((q0, k0), sb_w, 0, z * z_rows, z_rows),
        ((v0,), sb_w, 2, y * y_rows, y_rows),
        ((q1, k1, v1), delta_w, 0, y * y_rows, y_rows),
    )
    first = {}
    own = []

    def pass_on(s, d):
        mats, held, place, row, count = sets[s]
        to = at("fs", nx, d)
        first[s, d] = links.number()
        for m, w in enumerate(mats):
            src = w.at[pl.ds(row, count), pl.ds(pl.multiple_of(to * lanes, lanes), lanes)]
            cols = slice((place + m) * lanes, (place + m + 1) * lanes)
            dst = held.at[x, pl.ds(row, count), cols]
            if d:
                links.start(src, dst, first[s, d], "fs", to)
            else:
                own.append(pltpu.make_async_copy(src, dst, local.at[6 + len(own)]))
                own[-1].start()

    for d in (2, 1, 3, 0):
        pass_on(0, d)
        pass_on(1, d)
    for d in (2, 1, 3, 0):
        pass_on(2, d)
    right, left, other = at("fs", nx, 1), at("fs", nx, -1), 1 - t
    act = links.number(8)
    links.start(hidden_ref, acts.at[x, t], act, "fs", right)
    links.start(hidden_ref, acts.at[x, t], act + 1, "fs", left)
    links.start(hidden_ref, acts.at[x, t], act + 4, "tp", other)
    keep = pltpu.make_async_copy(hidden_ref, acts.at[x, t], local.at[12])
    keep.start()
    loads = [
        pltpu.make_async_copy(sb_out_ref, sb_out_w, local.at[0]),
        pltpu.make_async_copy(delta_out_ref, delta_out_w, local.at[1]),
    ]
    for s in range(nx):
        shift_out[s] = shift_in[s : s + 1]
    gates = jnp.concatenate(
        [
            decay_ref[...].astype(jnp.float32),
            write_ref[...].astype(jnp.float32),
            jnp.zeros((lanes - 2 * nx, decay_ref.shape[1]), jnp.float32),
        ],
        axis=0,
    )
    delta_w[:, :, width : width + lanes] = low(gates.T).reshape(nx, -1, lanes)
    row_at = lax.broadcasted_iota(jnp.int32, (tile, tile), 0)
    col_at = lax.broadcasted_iota(jnp.int32, (tile, tile), 1)
    later_ref[...] = jnp.where(row_at > col_at, 1.0, 0.0).astype(jnp.bfloat16)
    offset = jnp.full((tile, extra), offset_ref[2 * x + lax.rem(z, 2)], jnp.float32)
    parts = []
    for _ in range(3):
        parts.append(low(offset).astype(jnp.float32))
        offset = offset - parts[-1]
    part_at = lax.broadcasted_iota(jnp.int32, (tile, extra), 1)
    offset_part = jnp.zeros((tile, extra), jnp.float32)
    for k in range(3):
        offset_part = jnp.where(part_at == k, parts[k], offset_part)
    for row in range(nz):
        kv_ref[row, 2 * size : 2 * size + extra, :] = jnp.ones(
            (extra, kv_ref.shape[2]), jnp.bfloat16
        )

    z_right, z_left = at("sp_0", nz, 1), at("sp_0", nz, -1)
    y_right, y_left = at("sp_1", ny, 1), at("sp_1", ny, -1)
    steps = nz // 2
    zr, zl = links.number(steps), links.number(steps)
    vr, vl, dr, dl = (links.number(2) for _ in range(4))

    def sb_piece(by, lo=0, count=nx):
        rows = pl.ds(at("sp_0", nz, by) * z_rows, z_rows)
        return sb_w.at[lo : lo + count, rows, 0 : 2 * lanes]

    def v_piece(by, lo=0, count=nx):
        rows = pl.ds(at("sp_1", ny, by) * y_rows, y_rows)
        return sb_w.at[lo : lo + count, rows, 2 * lanes : width]

    def delta_piece(by, lo=0, count=nx):
        rows = pl.ds(at("sp_1", ny, by) * y_rows, y_rows)
        return delta_w.at[lo : lo + count, rows, 0:width]

    def come(s, rows):
        mats, held, place, row, count = sets[s]
        for d in (1, 3, 2):
            links.arrived(
                held.at[
                    at("fs", nx, -d), pl.ds(row, count),
                    place * lanes : (place + len(mats)) * lanes,
                ],
                first[s, d], "fs",
            )

    def y_start(piece, r, l):
        links.start(piece(0), piece(0), r, "sp_1", y_right)
        links.start(piece(0), piece(0), l, "sp_1", y_left)

    def y_step(piece, r, l):
        links.arrived(piece(-1), r, "sp_1")
        links.start(piece(-1, 0, 2), piece(-1, 0, 2), r + 1, "sp_1", y_right)
        links.arrived(piece(1), l, "sp_1")
        links.start(piece(1, 2, 2), piece(1, 2, 2), l + 1, "sp_1", y_left)

    def y_end(piece, r, l):
        links.arrived(piece(2, 0, 2), r + 1, "sp_1")
        links.arrived(piece(2, 2, 2), l + 1, "sp_1")

    def z_step(s):
        if s < steps:
            lo, count = (0, nx) if s < steps - 1 else (0, nx // 2)
            links.arrived(sb_piece(-s), zr + s - 1, "sp_0")
            links.start(sb_piece(-s, lo, count), sb_piece(-s, lo, count), zr + s, "sp_0", z_right)
            lo, count = (0, nx) if s < steps - 1 else (nx // 2, nx // 2)
            links.arrived(sb_piece(s), zl + s - 1, "sp_0")
            links.start(sb_piece(s, lo, count), sb_piece(s, lo, count), zl + s, "sp_0", z_left)
        else:
            links.arrived(sb_piece(steps, 0, nx // 2), zr + s - 1, "sp_0")
            links.arrived(sb_piece(steps, nx // 2, nx // 2), zl + s - 1, "sp_0")

    for made in own:
        made.wait()
    come(0, z_rows)
    links.start(sb_piece(0), sb_piece(0), zr, "sp_0", z_right)
    links.start(sb_piece(0), sb_piece(0), zl, "sp_0", z_left)
    come(1, y_rows)
    y_start(v_piece, vr, vl)
    shifts = links.number(nx)
    for d in range(1, nx):
        to = at("fs", nx, d)
        links.start(shift_out.at[to], shift_ref.at[x], shifts + d, "fs", to)
    keep_shift = pltpu.make_async_copy(shift_out.at[x], shift_ref.at[x], local.at[13])
    keep_shift.start()
    come(2, y_rows)
    y_start(delta_piece, dr, dl)
    z_step(1)
    y_step(v_piece, vr, vl)
    z_step(2)
    before, after, far = at("fs", nx, -1), at("fs", nx, 1), at("fs", nx, 2)
    links.arrived(acts.at[before, t], act, "fs")
    links.start(acts.at[before, t, 0:half], acts.at[before, t, 0:half], act + 2, "fs", right)
    links.start(acts.at[before, t], acts.at[before, t], act + 5, "tp", other)
    links.arrived(acts.at[after, t], act + 1, "fs")
    links.start(
        acts.at[after, t, half:tokens], acts.at[after, t, half:tokens], act + 3, "fs", left
    )
    links.start(acts.at[after, t], acts.at[after, t], act + 6, "tp", other)
    for made in loads:
        made.start()
    z_step(3)
    y_step(delta_piece, dr, dl)
    y_end(v_piece, vr, vl)
    z_step(4)
    keep.wait()

    def product(c, held):
        return sum(
            jnp.dot(
                acts[c, p],
                held[2 * p : 2 * p + 2].reshape(acts.shape[3], -1),
                preferred_element_type=jnp.float32,
            )
            for p in range(2)
        )

    def sb_sequence(c):
        out = product(c, sb_w)
        for m, place in enumerate((0, 2, 1)):
            block = low(out[:, m * lanes : (m + 1) * lanes].T)
            rows = slice(place * size, (place + 1) * size)
            units[2 * c, rows, :] = block[0:size]
            units[2 * c + 1, rows, :] = block[size:lanes]

    def delta_sequence(c):
        out = product(c, delta_w)
        delta_ref[c] = low(out[:, 0:width])
        pre_ref[c] = out[:, width : width + lanes].T[0:8]

    def near(i, carried):
        c = lax.rem(x + i + nx - 1, nx)
        sb_sequence(c)
        return carried

    for k, c in enumerate((x, before, after)):
        links.arrived(acts.at[c, other], act + 4 + k, "tp")
    lax.fori_loop(0, 3, near, 0)
    links.arrived(acts.at[far, t, 0:half], act + 2, "fs")
    links.arrived(acts.at[far, t, half:tokens], act + 3, "fs")
    links.start(acts.at[far, t], acts.at[far, t], act + 7, "tp", other)
    y_end(delta_piece, dr, dl)
    links.arrived(acts.at[far, other], act + 7, "tp")
    lax.fori_loop(3, 4, near, 0)
    delta_sequence(x)

    here = pl.ds(pl.multiple_of(y * tokens, tokens), tokens)
    zq, zk = links.number(nz), links.number(nz)
    order = (4, 3, 5, 2, 6, 1, 7)
    mine_units = (
        pltpu.make_async_copy(units.at[z, 0:size], query_ref.at[z], local.at[14]),
        pltpu.make_async_copy(units.at[z, size : 3 * size], kv_ref.at[z, 0 : 2 * size, here], local.at[15]),
    )
    for d in order:
        to = at("sp_0", nz, d)
        links.start(units.at[to, size : 3 * size], kv_ref.at[z, 0 : 2 * size, here], zk + d, "sp_0", to)
    for made in mine_units:
        made.start()
    for d in order:
        to = at("sp_0", nz, d)
        links.start(units.at[to, 0:size], query_ref.at[z], zq + d, "sp_0", to)

    kv_r, kv_l = links.number(nz), links.number(nz)
    kv_rr, kv_ll = links.number(nz), links.number(nz)

    def kv_piece(row, by, lo=0, count=2 * size):
        cols = pl.ds(pl.multiple_of(at("sp_1", ny, by) * tokens, tokens), tokens)
        return kv_ref.at[row, lo : lo + count, cols]

    def give(d):
        row = at("sp_0", nz, -d)
        if d:
            links.arrived(kv_ref.at[row, 0 : 2 * size, here], zk + d, "sp_0")
        links.start(kv_piece(row, 0), kv_piece(row, 0), kv_r + d, "sp_1", y_right)
        links.start(kv_piece(row, 0), kv_piece(row, 0), kv_l + d, "sp_1", y_left)

    def forward(d):
        row = at("sp_0", nz, -d)
        links.arrived(kv_piece(row, -1), kv_r + d, "sp_1")
        links.start(
            kv_piece(row, -1, 0, size), kv_piece(row, -1, 0, size), kv_rr + d, "sp_1", y_right
        )
        links.arrived(kv_piece(row, 1), kv_l + d, "sp_1")
        links.start(
            kv_piece(row, 1, size, size), kv_piece(row, 1, size, size), kv_ll + d, "sp_1", y_left
        )

    def delta_next(i, carried):
        delta_sequence(lax.rem(x + i, nx))
        return carried

    for made in mine_units:
        made.wait()
    give(0)
    lax.fori_loop(1, nx, delta_next, 0)
    keep_shift.wait()
    for d in range(1, nx):
        links.arrived(shift_ref.at[at("fs", nx, -d)], shifts + d, "fs")

    def mul(a, b, contract=((1,), (0,))):
        return lax.dot_general(
            low(a), low(b), (contract, ((), ())), preferred_element_type=jnp.float32
        )

    same = row_at // BLOCK == col_at // BLOCK
    inclusive = same & (col_at <= row_at)
    strictly = same & (col_at < row_at)
    decay_pre = jnp.concatenate([pre_ref[s, pl.ds(x, 1)] for s in range(nx)], axis=0)
    write_pre = jnp.concatenate([pre_ref[s, pl.ds(nx + x, 1)] for s in range(nx)], axis=0)
    shift = jnp.concatenate([shift_ref[s] for s in range(nx)], axis=0)
    softplus = jnp.maximum(decay_pre, 0.0) + jnp.log1p(jnp.exp(-jnp.abs(decay_pre)))
    rate = jnp.exp(jnp.full(decay_pre.shape, scale_ref[x], jnp.float32))
    log_decay = shift - rate * softplus
    strength = jax.nn.sigmoid(write_pre + bias_ref[x])
    up_to = jnp.where(same & (row_at <= col_at), 1.0, 0.0)
    both = jnp.concatenate([log_decay, strength], axis=0)
    summed = jnp.dot(
        both, up_to, preferred_element_type=jnp.float32, precision=lax.Precision.HIGHEST
    )
    sums_col = summed.T
    both_col = both.T
    blocks = tile // BLOCK

    def local_part(s):
        cum_row = summed[s : s + 1]
        cum = sums_col[:, s : s + 1]
        beta = both_col[:, nx + s : nx + s + 1]
        act = jax.nn.silu(delta_ref[s].astype(jnp.float32))
        q, k, v = act[:, 0:key], act[:, key : 2 * key], act[:, 2 * key : 3 * key]
        q = unit_rows(q) * key ** (-0.5)
        k = unit_rows(k)
        spread = cum - cum_row
        decay = jnp.where(inclusive, jnp.exp(jnp.where(inclusive, spread, 0.0)), 0.0)
        k_beta = k * beta
        lower = jnp.where(strictly, mul(k_beta, k, ((1,), (1,))) * decay, 0.0)
        inside = mul(q, k, ((1,), (1,))) * decay
        powered = lower
        inverse = jnp.where(row_at == col_at, 1.0, 0.0) - lower
        for _ in range(max(1, (BLOCK - 1).bit_length()) - 1):
            powered = mul(powered, powered)
            inverse = inverse + mul(inverse, powered)
        growth = jnp.exp(cum)
        updates = mul(inverse, jnp.concatenate([v * beta, k_beta * growth], axis=1))
        within = mul(inside, updates)
        reach = q * growth - within[:, key:]
        last = [cum[(b + 1) * BLOCK - 1 : (b + 1) * BLOCK] for b in range(blocks)]
        carried = None
        eye = jnp.where(
            lax.broadcasted_iota(jnp.int32, (key, key), 0)
            == lax.broadcasted_iota(jnp.int32, (key, key), 1),
            1.0,
            0.0,
        )
        zero = jnp.zeros((key, key), jnp.float32)
        for b in range(blocks):
            rows = slice(b * BLOCK, (b + 1) * BLOCK)
            damped = k[rows] * jnp.exp(last[b] - cum[rows])
            step = mul(damped, updates[rows], ((0,), (0,)))
            keep = jnp.exp(last[b])
            start = jnp.concatenate([zero, eye], axis=1) if carried is None else carried
            out = mul(reach[rows], start)
            local_out[s, rows] = within[rows, 0:key] + out[:, 0:key]
            through[s, rows] = low(out[:, key:])
            carried = (
                start * keep
                - mul(step[:, key:], start)
                + jnp.concatenate([step[:, 0:key], zero], axis=1)
            )
        transfer[s] = low(carried)

    give(4)
    local_part(0)
    give(3)
    give(5)
    forward(0)
    local_part(1)
    give(2)
    give(6)
    forward(4)
    forward(3)
    local_part(2)
    give(1)
    give(7)
    forward(5)
    forward(2)
    local_part(3)
    forward(6)
    forward(1)
    forward(7)

    one = links.number(ny)
    for d in (2, 1, 3):
        to = at("sp_1", ny, d)
        links.start(transfer.at[to], stage1.at[y], one + d, "sp_1", to)
    mine = pltpu.make_async_copy(transfer.at[y], stage1.at[y], local.at[2])
    mine.start()
    for d in (0,) + order:
        row = at("sp_0", nz, -d)
        if d:
            links.arrived(query_ref.at[row], zq + d, "sp_0")
        links.arrived(kv_piece(row, 2, 0, size), kv_rr + d, "sp_1")
        links.arrived(kv_piece(row, 2, size, size), kv_ll + d, "sp_1")
    two, three = links.number(nz), links.number(ny)
    keep_own = pltpu.make_async_copy(leaving.at[y], incoming.at[y], local.at[3])

    def over_group():
        mine.wait()
        for d in range(1, ny):
            links.arrived(stage1.at[at("sp_1", ny, -d)], one + d, "sp_1")
        joined = stage1[0].astype(jnp.float32)
        for k in range(1, ny):
            own = stage1[k]
            new = mul(own[:, key:], joined)
            joined = jnp.concatenate(
                [new[:, 0:key] + own[:, 0:key].astype(jnp.float32), new[:, key:]], axis=1
            )
        stage2[z] = low(joined)

    def share_group():
        for d in (4, 3, 5, 2, 6, 1, 7):
            links.start(stage2.at[z], stage2.at[z], two + d, "sp_0", at("sp_0", nz, d), lambda: stage2.at[0])

    def over_line():
        for d in range(1, nz):
            links.arrived(stage2.at[at("sp_0", nz, -d)], two + d, "sp_0")
        state = jnp.zeros((key, key), jnp.float32)
        for k in range(nz - 1):
            own = stage2[k]
            new = mul(own[:, key:], state) + own[:, 0:key].astype(jnp.float32)
            state = jnp.where(k < z, new, state)
        for k in range(ny):
            leaving[k] = low(state)
            if k < ny - 1:
                own = stage1[k]
                state = mul(own[:, key:], state) + own[:, 0:key].astype(jnp.float32)

    def share_states():
        for d in (2, 1, 3):
            to = at("sp_1", ny, d)
            links.start(leaving.at[to], incoming.at[y], three + d, "sp_1", to, lambda: leaving.at[0])
        keep_own.start()

    def delta_end():
        keep_own.wait()
        for d in range(1, ny):
            links.arrived(incoming.at[at("sp_1", ny, -d)], three + d, "sp_1")
        for s in range(nx):
            rows = mul(through[s], incoming[s]) + local_out[s]
            normed = (
                rows
                * lax.rsqrt(jnp.mean(rows * rows, axis=-1, keepdims=True) + NORM_EPS)
                * gain_ref[...]
            )
            delta_done[s] = low(normed)

    four = links.number(nx)
    keep_delta = pltpu.make_async_copy(delta_done.at[x], delta_in.at[x], local.at[4])

    def share_delta():
        for d in (2, 1, 3):
            to = at("fs", nx, d)
            links.start(delta_done.at[to], delta_in.at[x], four + d, "fs", to, lambda: delta_done.at[0])
        keep_delta.start()

    def key_row(row, count, diagonal):
        queries = rows_ref[...]
        beyond = None if diagonal else beyond_ref[...]
        weights = []
        for k in range(count - 1, -1, -1):
            scores = jnp.dot(
                queries,
                kv_ref[row, size : 2 * size + extra, k * tile : (k + 1) * tile],
                preferred_element_type=jnp.float32,
            )
            above = jnp.maximum(scores, 0.0)
            below = scores - above
            small = jnp.exp(below - above)
            log_term = jnp.where(small < 2.0**-12, small, jnp.log(1.0 + small))
            passed = above + log_term
            exponent = below - log_term
            if diagonal and k == count - 1:
                visible = col_at < row_at
                passed = jnp.where(visible, passed, 0.0)
                exponent = jnp.where(visible, exponent, -jnp.inf)
            after = jnp.dot(low(passed), later_ref[...], preferred_element_type=jnp.float32)
            exponent = exponent - after
            if beyond is not None:
                exponent = exponent - beyond
            total = after[:, :1] + passed[:, :1]
            beyond = total if beyond is None else beyond + total
            weights.append(low(jnp.exp(exponent)))
        partial = lax.dot_general(
            kv_ref[row, 0:size, 0 : count * tile],
            jnp.concatenate(weights[::-1], axis=1),
            (((1,), (1,)), ((), ())),
            preferred_element_type=jnp.float32,
        )
        beyond_ref[...] = beyond
        if diagonal:
            acc_ref[...] = partial
        else:
            acc_ref[...] += partial

    five = links.number(2 * nx)
    sends = links.sent
    links.sent += nz
    home = z // 2
    slot = 2 * x + lax.rem(z, 2)

    def sb_copy(row):
        return pltpu.make_async_remote_copy(
            src_ref=done_ref.at[row],
            dst_ref=sb_in.at[slot],
            send_sem=send.at[sends + row],
            recv_sem=recv.at[five + slot],
            device_id={"fs": home, "sp_0": row},
            device_id_type=pl.DeviceIdType.MESH,
        )

    keep_sb = pltpu.make_async_copy(done_ref.at[z], sb_in.at[slot], local.at[5])

    def send_back(row):
        stays = (row == z) & (home == x)

        @pl.when(stays)
        def _():
            keep_sb.start()

        @pl.when(jnp.logical_not(stays))
        def _():
            sb_copy(row).start()

    def per_query(row, unused):
        scaled = (query_ref[row].astype(jnp.float32) * size ** (-0.5)).T
        rows_ref[...] = low(jnp.concatenate([scaled, offset_part], axis=1))
        pl.when(row == 3)(over_group)
        pl.when(row == 6)(over_line)
        pl.when(row == 7)(delta_end)
        for k in range(groups):

            @pl.when(y == k)
            def _():
                key_row(row, k + 1, True)

        pl.when(row == 3)(share_group)
        pl.when(row == 6)(share_states)
        pl.when(row == 7)(share_delta)

        @pl.when(row > 0)
        def _():
            send_back(row - 1)

        def earlier(step, carried):
            key_row(row - 1 - step, groups, False)
            return carried

        lax.fori_loop(0, row, earlier, 0)
        done_ref[row] = low(acc_ref[...])
        return unused

    lax.fori_loop(0, nz, per_query, 0)
    for made in loads:
        made.wait()
    send_back(nz - 1)
    keep_delta.wait()
    for d in range(1, nx):
        links.arrived(delta_in.at[at("fs", nx, -d)], four + d, "fs")

    rows = tile // 2
    mine_rows = pl.ds(pl.multiple_of(t * rows, rows), rows)
    other_rows = pl.ds(pl.multiple_of((1 - t) * rows, rows), rows)
    delta_mixed = [delta_in[k] for k in range(nx)]
    columns = result_ref.shape[1]
    span = columns // 4
    for k in range(nx):
        for h in range(2):
            here = (z == 2 * x + h) & (x == k)

            @pl.when(here)
            def _():
                keep_sb.wait()

            @pl.when(jnp.logical_not(here))
            def _():
                links.arrived(sb_in.at[2 * k + h], five + 2 * k + h, "fs")

    sb_rows = sb_in[...].reshape(nz * size, tile).astype(jnp.float32).T
    rows_ref2 = low(jnp.concatenate([sb_rows] + [d.astype(jnp.float32) for d in delta_mixed], axis=1))
    taken[...] = rows_ref2
    six = links.number(4)

    def projected(part, cols):
        return low(
            jnp.dot(
                taken[part, 0 : nz * size], sb_out_w[:, cols], preferred_element_type=jnp.float32
            )
            + jnp.dot(
                taken[part, nz * size :], delta_out_w[:, cols], preferred_element_type=jnp.float32
            )
        )

    outs = [slice(c * span, (c + 1) * span) for c in range(4)]
    for c in range(4):
        given[0, :, outs[c]] = projected(other_rows, outs[c])
        if c:
            links.start(
                given.at[0, :, outs[c - 1]], given.at[1, :, outs[c - 1]], six + c - 1, "tp", 1 - t
            )
    own = projected(mine_rows, outs[0])
    links.start(given.at[0, :, outs[3]], given.at[1, :, outs[3]], six + 3, "tp", 1 - t)
    for c in range(4):
        links.arrived(given.at[1, :, outs[c]], six + c, "tp")
        total = own.astype(jnp.float32) + given[1, :, outs[c]].astype(jnp.float32)
        result_ref[:, outs[c]] = low(total)
        if c < 3:
            own = projected(mine_rows, outs[c + 1])
    for row in range(nz):

        @pl.when(jnp.logical_not((row == z) & (home == x)))
        def _():
            sb_copy(row).wait_send()

    links.drain()


def layer(offset, bias, scale, hidden, decay, write, shift, gain, sb_w, delta_w, sb_out, delta_out):
    nz, ny, nx = (lax.axis_size(a) for a in ("sp_0", "sp_1", "fs"))
    tile, part = hidden.shape
    rows, lanes = sb_w[0].shape[0], sb_w[0].shape[1] // nx
    size, key = lanes // 2, lanes
    columns = sb_out.shape[1]
    half = tile // 2
    smem = pl.BlockSpec(memory_space=pltpu.SMEM)
    vmem = pl.BlockSpec(memory_space=pltpu.VMEM)
    anywhere = pl.BlockSpec(memory_space=pl.ANY)
    copies = 160
    bf16, f32 = jnp.bfloat16, jnp.float32
    return pl.pallas_call(
        layer_kernel,
        out_shape=jax.ShapeDtypeStruct((half, columns), bf16),
        in_specs=[smem] * 3 + [vmem] * 5 + [anywhere] * 8,
        out_specs=vmem,
        scratch_shapes=[
            pltpu.VMEM((nx, 2, tile, part), bf16),
            pltpu.VMEM((nx, rows, 3 * lanes), bf16),
            pltpu.VMEM((nx, rows, 4 * lanes), bf16),
            pltpu.VMEM((nz, 3 * size, tile), bf16),
            pltpu.VMEM((nz, size, tile), bf16),
            pltpu.VMEM((nz, 2 * size + 16, ny * tile), bf16),
            pltpu.VMEM((nx, tile, 3 * key), bf16),
            pltpu.VMEM((nx, 8, tile), f32),
            pltpu.VMEM((nx, 1, tile), f32),
            pltpu.VMEM((nx, 1, tile), f32),
            pltpu.VMEM((tile, tile), bf16),
            pltpu.VMEM((tile, size + 16), bf16),
            pltpu.VMEM((size, tile), f32),
            pltpu.VMEM((tile, 1), f32),
            pltpu.VMEM((nz, size, tile), bf16),
            pltpu.VMEM((2 * nx, size, tile), bf16),
            pltpu.VMEM((nx, tile, key), bf16),
            pltpu.VMEM((nx, tile, key), bf16),
            pltpu.VMEM((nx, tile, key), bf16),
            pltpu.VMEM((nx, tile, key), f32),
            pltpu.VMEM((nx, key, 2 * key), bf16),
            pltpu.VMEM((ny, key, 2 * key), bf16),
            pltpu.VMEM((nz, key, 2 * key), bf16),
            pltpu.VMEM((ny, key, key), bf16),
            pltpu.VMEM((nx, key, key), bf16),
            pltpu.VMEM(sb_out.shape, bf16),
            pltpu.VMEM(delta_out.shape, bf16),
            pltpu.VMEM((2, half, columns), bf16),
            pltpu.VMEM((tile, nz * size + nx * key), bf16),
            pltpu.SemaphoreType.DMA((copies,)),
            pltpu.SemaphoreType.DMA((copies,)),
            pltpu.SemaphoreType.DMA((16,)),
        ],
        compiler_params=pltpu.CompilerParams(collective_id=0, has_side_effects=True),
        name="layer",
    )(offset, bias, scale, hidden, decay, write, shift, gain, *sb_w, *delta_w, sb_out, delta_out)


def on_device(
    hidden_in,
    sb_query_w,
    sb_key_w,
    sb_value_w,
    sb_offset,
    delta_query_w,
    delta_key_w,
    delta_value_w,
    decay_w,
    write_w,
    write_bias,
    decay_log_scale,
    decay_shift,
    head_gain,
    sb_out_w,
    delta_out_w,
):
    tokens, part = hidden_in.shape[1], hidden_in.shape[2]
    result = layer(
        sb_offset,
        write_bias,
        decay_log_scale,
        hidden_in.reshape(tokens, part),
        decay_w.T,
        write_w.T,
        decay_shift.reshape(-1, tokens),
        head_gain.reshape(1, -1),
        (sb_query_w, sb_key_w, sb_value_w),
        (delta_query_w, delta_key_w, delta_value_w),
        sb_out_w,
        delta_out_w,
    )
    return result.reshape(1, *result.shape)


def solution(mesh):
    finer = Mesh(
        mesh.devices.reshape(8, 4, mesh.shape["fs"], mesh.shape["tp"]), ("sp_0", "sp_1", "fs", "tp")
    )
    return jax.shard_map(
        on_device,
        mesh=finer,
        in_specs=(
            P("fs", SP, "tp"),
            P("fs", "tp"),
            P("fs", "tp"),
            P("fs", "tp"),
            P("tp"),
            P("fs", "tp"),
            P("fs", "tp"),
            P("fs", "tp"),
            P(None, "tp"),
            P(None, "tp"),
            P("tp"),
            P("tp"),
            P("fs", "tp", SP),
            P(),
            P("tp", None),
            P("tp", None),
        ),
        out_specs=P("fs", SP_TP, None),
        check_vma=False,
    )
```
